32 devices in a mesh: grp: 2 (over y), sp: 4 (over z), tp: 4 (over x, core).
Axes of the slice: x: 2, y: 2, z: 4, core: 2. Of those that a mesh axis runs over, the one named last changes fastest.
Arguments:
- tokens: bfloat16 [16384, 2048], P(('grp', 'sp')), parts along dimension 0, may hold values from -6 to 6
- in_gain: float32 [2048], replicated, may hold values from 0.1 to 1.9
- w_input: bfloat16 [2048, 2048], P(None, 'tp'), may hold values from -0.125 to 0.125
- w_gate: bfloat16 [2048, 2048], P(None, 'tp'), may hold values from -4 to 4
- conv_taps: float32 [4, 2048], P(None, 'tp'), may hold values from -3 to 3
- w_rate: bfloat16 [8, 256, 256], P('tp'), may hold values from -0.375 to 0.375
- w_inlet: bfloat16 [8, 256, 256], P('tp'), may hold values from -0.375 to 0.375
- decay_param: float32 [2048], P('tp'), may hold values from 3 to 25
- decay_bias: float32 [8, 16384], P('tp', ('grp', 'sp')), parts along dimension 1, may hold values from -1.5 to 0
- out_gain: float32 [2048], P('tp'), may hold values from 0.1 to 1.9
- w_out: bfloat16 [2048, 2048], P('sp'), may hold values from -0.125 to 0.125
Outputs:
- mixer_out: bfloat16 [16384, 2048], P(('grp', 'sp', 'tp')), parts along dimension 0
The draws below stay inside these ranges and needn't reach their ends.
There are 2 independent parts, one for each index of `grp`. The reference program is written for one: setup_inputs(seed, part) draws one part's arguments, and reference() takes and returns one part's arrays. A program takes and returns all parts, laid end to end along the dimension named above; an argument that names none is the same for every part. Nothing has to cross between parts.
All inputs are finite; a program needn't handle non-finite values.
Results may differ from the reference program's by a relative error of at most 0.013.
Values may be sent and summed in bfloat16 or wider, within the bound.
A program may use at most 128 MiB of HBM per device.

```python
import math
import jax
import jax.numpy as jnp
from jax import lax

D = 2048
HEADS = 8
HEAD = 256
CONV = 4
SEQ_DEV = 2048
DR = 2048
SEQ = 8192


def draw_w_gate(key, part):
    base_key, jitter_key = jax.random.split(jax.random.fold_in(key, 11))
    columns = HEADS * HEAD
    base = jnp.clip(jax.random.normal(base_key, (D, columns), jnp.float32), -4.0, 4.0)
    position = jnp.arange(columns, dtype=jnp.float32) / columns
    jitter = jax.random.uniform(jitter_key, (columns,), jnp.float32) / HEADS
    column_scale = jnp.exp((position + jitter) * math.log(6.0))
    return (base * column_scale[None, :] / math.sqrt(D)).astype(jnp.bfloat16)


def draw_decay_param(key, part):
    pick_key, slow_key, fast_key = jax.random.split(jax.random.fold_in(key, 23), 3)
    channels = HEADS * HEAD
    slow = jax.random.bernoulli(pick_key, 0.5, (channels,))
    slow_rate = jax.random.uniform(slow_key, (channels,), jnp.float32, 0.2, 0.6) / (8.0 * SEQ)
    fast_rate = jnp.exp(jax.random.uniform(fast_key, (channels,), jnp.float32, math.log(1.0 / 400.0), math.log(1.0 / 120.0)))
    chosen = jnp.where(slow, slow_rate, fast_rate)
    return -jnp.log(jnp.expm1(chosen))


def draw_decay_bias(key, part):
    span_key, spot_key, depth_key = jax.random.split(jax.random.fold_in(key, 37), 3)
    span_count = SEQ // SEQ_DEV
    level = jnp.exp(jax.random.uniform(span_key, (HEADS, span_count), jnp.float32, math.log(0.2), math.log(1.2))) / SEQ
    dispersion = jnp.repeat(-level, SEQ_DEV, axis=1)
    spots = jax.random.randint(spot_key, (HEADS, 2), 0, SEQ)
    layer_count = jnp.log(jax.random.uniform(depth_key, (HEADS, 2), jnp.float32, 0.55, 0.8))
    match_count = (jnp.arange(SEQ, dtype=jnp.int32)[None, None, :] == spots[:, :, None]).astype(jnp.float32)
    pulse_train = jnp.sum(match_count * layer_count[:, :, None], axis=1)
    return dispersion + pulse_train


def level_of(key, dims, shards, least, top_value):
    factor_of = 1.0
    for dim, parts in shards:
        heights = jax.random.uniform(jax.random.fold_in(jax.random.fold_in(key, 6), dim), (parts,), jnp.float32, least / len(shards), top_value / len(shards))
        factor_of = factor_of * jnp.repeat(jnp.exp(heights), dims[dim] // parts).reshape((-1,) + (1,) * (len(dims) - 1 - dim))
    return factor_of


def scatter_about(key, dims, deviation, reach, shards=(), held_as=jnp.bfloat16):
    factor_of = level_of(key, dims, shards, -0.22, 0.18) if shards else 1.0
    drawn = jax.random.normal(key, dims, jnp.float32) * deviation * factor_of
    return jnp.minimum(jnp.maximum(drawn, -reach), reach).astype(held_as)


def setup_inputs(seed: int = 0, part: int = 0) -> dict:
    key_of = jax.random.split(jax.random.key(seed), 12)
    own_keys = jax.random.split(jax.random.fold_in(key_of[11], part), 12)
    return {
        "tokens": scatter_about(own_keys[0], (SEQ, D), 1.0, 6.0, ((0, 4),)),
        "in_gain": jnp.clip(1.0 + 0.18 * jax.random.normal(key_of[1], (D,), jnp.float32), 0.1, 1.9),
        "w_input": scatter_about(key_of[2], (D, DR), D ** -0.5, 0.125, ((1, 4),)),
        "w_gate": draw_w_gate(jax.random.fold_in(key_of[11], 71), part),
        "conv_taps": scatter_about(key_of[4], (CONV, DR), 0.5, 3.0, ((1, 4),), jnp.float32),
        "w_rate": scatter_about(key_of[5], (HEADS, HEAD, HEAD), HEAD ** -0.5, 0.375, ((0, 4),)),
        "w_inlet": scatter_about(key_of[6], (HEADS, HEAD, HEAD), HEAD ** -0.5, 0.375, ((0, 4),)),
        "decay_param": draw_decay_param(jax.random.fold_in(key_of[11], 71), part),
        "decay_bias": draw_decay_bias(jax.random.fold_in(jax.random.fold_in(key_of[11], part), 71), part),
        "out_gain": jnp.clip(1.0 + 0.18 * jax.random.normal(key_of[9], (DR,), jnp.float32), 0.1, 1.9),
        "w_out": scatter_about(key_of[10], (DR, D), DR ** -0.5, 0.125, ((0, 4),)),
    }


def combine_pairs(first_pair, second_pair):
    return (first_pair[0] * second_pair[0], second_pair[0] * first_pair[1] + second_pair[1])

def reference(tokens, in_gain, w_input, w_gate, conv_taps, w_rate, w_inlet, decay_param, decay_bias, out_gain, w_out):
    seq_len = tokens.shape[0]
    as_float = tokens.astype(jnp.float32)
    inv_norm = lax.rsqrt(lax.optimization_barrier(jnp.mean(as_float * as_float, axis=1, keepdims=True)) + 1e-06)
    normed = (as_float * inv_norm * in_gain).astype(jnp.bfloat16)
    projected = jnp.dot(normed, w_input, preferred_element_type=jnp.float32).astype(jnp.bfloat16)
    gate_raw = jnp.dot(normed, w_gate, preferred_element_type=jnp.float32).astype(jnp.bfloat16)
    padded = jnp.pad(projected.astype(jnp.float32), ((CONV - 1, 0), (0, 0)))
    tap_values = conv_taps.astype(jnp.float32)
    summed = padded[0:seq_len] * tap_values[0]
    for offset in range(1, CONV):
        summed = summed + padded[offset:offset + seq_len] * tap_values[offset]
    convolved = summed.astype(jnp.bfloat16)
    per_head = convolved.astype(jnp.float32).reshape(seq_len, HEADS, HEAD)
    rate_gate = jax.nn.sigmoid(jnp.einsum('shi,hij->shj', per_head, w_rate.astype(jnp.float32))).reshape(seq_len, HEADS * HEAD)
    input_gate = jax.nn.sigmoid(jnp.einsum('shi,hij->shj', per_head, w_inlet.astype(jnp.float32))).reshape(seq_len, HEADS * HEAD)
    head_bias = jnp.repeat(jnp.transpose(decay_bias), HEAD, axis=1)
    log_decay = -8.0 * rate_gate * jax.nn.softplus(-decay_param) + head_bias
    drive_term = jnp.sqrt(-jnp.expm1(2.0 * log_decay)) * input_gate * convolved.astype(jnp.float32)
    decay_prod, full_state = lax.associative_scan(combine_pairs, (jnp.exp(log_decay), drive_term), axis=0)
    gated_out = full_state * jax.nn.gelu(gate_raw.astype(jnp.float32))
    out_scale = lax.rsqrt(lax.optimization_barrier(jnp.mean(gated_out * gated_out, axis=1, keepdims=True)) + 1e-06)
    normed_out = (gated_out * out_scale * out_gain).astype(jnp.bfloat16)
    return jnp.dot(normed_out, w_out, preferred_element_type=jnp.float32).astype(jnp.bfloat16)
```

```python
import functools
import math
import jax
import jax.numpy as jnp
from jax import lax
from jax.experimental import pallas as pl
from jax.experimental.pallas import tpu as pltpu
from jax.sharding import PartitionSpec as P

MESH = pl.DeviceIdType.MESH
F32 = jnp.float32
BF16 = jnp.bfloat16
CHUNK = 256
SEG = CHUNK // 8
STRIDE = SEG + 8
LANES = 128
LAG = 2
FIRST = 3
EVERY = 3
BEHIND = 4
AHEAD = 6
BETWEEN = 1
LN2 = math.log(2.0)
GELU_A = math.sqrt(2.0 / math.pi)
GELU_B = GELU_A * 0.044715


def gelu_half(value):
    inner = value * (GELU_A + GELU_B * (value * value))
    return (0.25 * value) * (1.0 + jnp.tanh(inner))


def softplus_of_minus(value):
    small = jnp.exp(-jnp.abs(value))
    z = small / (2.0 + small)
    zz = z * z
    series = 1.0 / 15.0
    for n in (13, 11, 9, 7, 5, 3, 1):
        series = series * zz + 1.0 / n
    return jnp.maximum(-value, 0.0) + 2.0 * z * series


def spread(row):
    return jnp.broadcast_to(row, (8, row.shape[1]))


def columns_of(row):
    return jnp.broadcast_to(row, (LANES, row.shape[1])).T


def kernel(
    sizes,
    tokens, in_gain, w_input, w_gate, taps, w_rate, w_inlet, decay_param, bias, out_gain, w_out,
    out,
    x, w_in, w_all, gates_w, inv, proj, graw, conv, raw, bias_p, scale_row, before,
    state, prod, gate, pre_s, pre_p, natural, gated, arrived, total, result, halo,
    squares, squares_in, ends, ends_in,
    x_sem, w_sem, out_load_sem, halo_send, halo_recv, z_send, z_recv, y_send, y_recv,
    m_send, m_recv, end_send, end_recv, a_send, a_recv, q_send, q_recv, own_sem, out_sem,
):
    n_grp, n_sp, n_tp = sizes
    grp, sp, tp = lax.axis_index("grp"), lax.axis_index("sp"), lax.axis_index("tp")
    rows, width = tokens.shape
    heads, head = w_rate.shape[0], w_rate.shape[1]
    parts = head // LANES
    channels = heads * head
    reach = taps.shape[0] - 1
    chunks = rows // CHUNK
    steps = heads * chunks
    out_rows = rows // n_tp
    per_owner = out_rows // CHUNK
    shard = w_out.shape[0]
    quarter = shard // (2 * n_grp)
    piece = max(16, quarter // 4)
    pieces = quarter // piece
    items = (n_sp - 1) * pieces
    core = lax.rem(tp, 2)
    mate = tp + 1 - 2 * core
    across = 1 - grp

    def x_copy(i):
        at = pl.ds(pl.multiple_of(i * CHUNK, CHUNK), CHUNK)
        return pltpu.make_async_copy(tokens.at[at], x.at[at], x_sem.at[i])

    def w_copies(h):
        lanes = pl.ds(h * head, head)
        return (
            pltpu.make_async_copy(w_input.at[:, lanes], w_in.at[h, :, 0:head], w_sem.at[2 * h]),
            pltpu.make_async_copy(
                w_gate.at[:, lanes], w_in.at[h, :, head : 2 * head], w_sem.at[2 * h + 1]
            ),
        )

    out_load = pltpu.make_async_copy(
        w_out, w_all.at[pl.ds(pl.multiple_of(sp * shard, shard), shard)], out_load_sem
    )

    ends_in[...] = jnp.zeros_like(ends_in)
    barrier = pltpu.get_barrier_semaphore()
    for d in range(1, n_sp):
        pl.semaphore_signal(
            barrier, inc=1, device_id={"sp": lax.rem(sp + d, n_sp)}, device_id_type=MESH
        )
    for k in range(1, n_tp):
        pl.semaphore_signal(
            barrier, inc=1, device_id={"tp": lax.rem(tp + k, n_tp)}, device_id_type=MESH
        )
    pl.semaphore_signal(barrier, inc=1, device_id={"grp": across}, device_id_type=MESH)

    for copy in w_copies(0):
        copy.start()
    x_copy(0).start()

    def remote(src, dst, send, recv, where):
        return pltpu.make_async_remote_copy(
            src_ref=src, dst_ref=dst, send_sem=send, recv_sem=recv,
            device_id=where, device_id_type=MESH,
        )

    halo_rows = halo.shape[0]
    halo_copy = remote(
        tokens.at[pl.ds(rows - halo_rows, halo_rows)], halo, halo_send, halo_recv,
        {"sp": jnp.minimum(sp + 1, n_sp - 1)},
    )

    def w_rows(source, which, p):
        first = source * shard + which * quarter + p * piece
        return w_all.at[pl.ds(pl.multiple_of(first, piece), piece)]

    def which_of(other, owner):
        return (across if other else grp) * 2 + owner

    def own_copy(to_right, p):
        mine = which_of(False, core)
        first = pl.multiple_of(mine * quarter + p * piece, piece)
        slot = ((0 if to_right else 1) * n_sp + sp) * pieces + p
        return remote(
            w_out.at[pl.ds(first, piece)], w_rows(sp, mine, p),
            z_send.at[slot], z_recv.at[sp * pieces + p],
            {"sp": jnp.minimum(sp + 1, n_sp - 1) if to_right else jnp.maximum(sp - 1, 0)},
        )

    def z_copy(source, p, to_right):
        at = w_rows(source, which_of(False, core), p)
        slot = ((0 if to_right else 1) * n_sp + source) * pieces + p
        return remote(
            at, at, z_send.at[slot], z_recv.at[source * pieces + p],
            {"sp": jnp.minimum(sp + 1, n_sp - 1) if to_right else jnp.maximum(sp - 1, 0)},
        )

    def y_copy(source, p, incoming=False):
        at = w_rows(source, which_of(incoming, core), p)
        slot = source * pieces + p
        return remote(at, at, y_send.at[slot], y_recv.at[slot], {"grp": across})

    def m_copy(source, p, second, incoming=False):
        at = w_rows(source, which_of(second, 1 - core if incoming else core), p)
        slot = ((1 if second else 0) * n_sp + source) * pieces + p
        return remote(at, at, m_send.at[slot], m_recv.at[slot], {"tp": mate})

    inner = jnp.minimum(sp, n_sp - 1 - sp)
    leftward = sp > n_sp - 1 - sp

    def source_of(b):
        d = jnp.where(b <= 2 * inner, (b + 1) // 2, b - inner)
        from_left = jnp.where(b <= 2 * inner, b % 2 == 1, leftward)
        return jnp.where(from_left, sp - d, sp + d)

    held = 2

    def each_source(n, action):
        d, p = 1 + n // pieces, n % pieces

        @pl.when(sp >= d)
        def _():
            action(sp - d, p, True)

        @pl.when(sp + d < n_sp)
        def _():
            action(sp + d, p, False)

    def onward(source, p, from_left, act):
        if from_left:
            pl.when(sp < n_sp - 1)(lambda: act(z_copy(source, p, True)))
        else:
            pl.when(sp > 0)(lambda: act(z_copy(source, p, False)))

    def take_z(source, p, from_left):
        z_copy(source, p, from_left).wait_recv()
        y_copy(source, p).start()
        m_copy(source, p, False).start()

    def take_y(source, p, from_left):
        y_copy(source, p, True).wait_recv()
        m_copy(source, p, True).start()

    def send_on(up, source, p, from_left):
        if up == from_left:
            onward(source, p, from_left, lambda copy: copy.start())

    def pump(n):
        @pl.when(n < items)
        def _():
            each_source(n, take_z)
            each_source(n, functools.partial(send_on, False))

        @pl.when((n >= held) & (n < items))
        def _():
            each_source(n, functools.partial(send_on, True))

        @pl.when(n == held)
        def _():
            for k in range(held):
                each_source(k, functools.partial(send_on, True))

        @pl.when(n >= LAG)
        def _():
            each_source(n - LAG, take_y)

    def fold(h):
        for copy in w_copies(h):
            copy.wait()

        def block(j, _):
            at = pl.ds(pl.multiple_of(j * CHUNK, CHUNK), CHUNK)
            gain = columns_of(in_gain[0:1, at])
            for c in range(2 * parts):
                lanes = slice(c * LANES, (c + 1) * LANES)
                w_in[h, at, lanes] = (w_in[h, at, lanes].astype(F32) * gain).astype(BF16)
            return 0

        lax.fori_loop(0, width // CHUNK, block, 0)

    def norm_of(chunk):
        as_float = chunk.astype(F32)
        return lax.rsqrt(jnp.mean(as_float * as_float, axis=1, keepdims=True) + 1e-06)

    def lanes_of(h, c):
        return pl.ds(pl.multiple_of(h * head + c * LANES, LANES), LANES)

    def project(s, sums):
        h, i = s // chunks, s % chunks
        at = pl.ds(pl.multiple_of(i * CHUNK, CHUNK), CHUNK)
        acc = jnp.dot(x[at, :], w_in[h], preferred_element_type=F32)
        if sums:
            scale = jnp.broadcast_to(norm_of(x[at, :]), (CHUNK, LANES))
            inv[at, :] = scale
        else:
            scale = inv[at, :]
        return acc, scale

    def keep(s, acc, scale):
        h, i = s // chunks, s % chunks
        for c in range(parts):
            last = proj[c, 7 * STRIDE + SEG : 8 * STRIDE, :]
            proj[c, 0:8, :] = jnp.where(i == 0, before[h, c], last)
            for g in range(8):
                at = slice(g * SEG, (g + 1) * SEG)
                block = acc[at, c * LANES : (c + 1) * LANES] * scale[at]
                proj[c, g * STRIDE + 8 : (g + 1) * STRIDE, :] = block
                if g < 7:
                    proj[c, (g + 1) * STRIDE : (g + 1) * STRIDE + 8, :] = block[SEG - 8 :]
                other = acc[at, head + c * LANES : head + (c + 1) * LANES] * scale[at]
                graw[c, g * STRIDE : g * STRIDE + SEG, :] = other

    def convolve(s):
        h, i = s // chunks, s % chunks
        for c in range(parts):
            lanes = lanes_of(h, c)
            tap = [spread(taps[k : k + 1, lanes]) for k in range(reach + 1)]
            window = [
                proj[c, pl.ds(8 - reach + j, 8, stride=STRIDE), :] for j in range(SEG + reach)
            ]
            done = []
            for k in range(SEG):
                summed = window[k] * tap[0]
                for j in range(1, reach + 1):
                    summed = summed + window[k + j] * tap[j]
                done.append(summed)
            for k in range(SEG):
                value = graw[c, pl.ds(k, 8, stride=STRIDE), :]
                gate[s, c, k * 8 : k * 8 + 8, :] = gelu_half(value)
            for k in range(0, SEG, 2):
                pair = jnp.concatenate(done[k : k + 2], axis=0).astype(BF16)
                conv[k * 8 : k * 8 + 16, c * LANES : (c + 1) * LANES] = pair
        row = bias[pl.ds(h, 1), pl.ds(pl.multiple_of(i * CHUNK, CHUNK), CHUNK)] * (1.0 / LN2)
        cols = columns_of(row)
        for g in range(8):
            bias_p[g * STRIDE : g * STRIDE + SEG, :] = cols[g * SEG : (g + 1) * SEG]
        raw[...] = jnp.dot(conv[...], gates_w[h], preferred_element_type=F32)

    sublane = lax.broadcasted_iota(jnp.int32, (8, LANES), 0)

    def elementwise(s, carry):
        h, i = s // chunks, s % chunks
        after = []
        for c in range(parts):
            scale = spread(scale_row[0:1, lanes_of(h, c)])
            lanes = slice(c * LANES, (c + 1) * LANES)
            st, pt = jnp.zeros((8, LANES), F32), jnp.ones((8, LANES), F32)
            for k in range(SEG):
                at = slice(k * 8, k * 8 + 8)
                if k % 2 == 0:
                    pair = conv[k * 8 : k * 8 + 16, lanes].astype(F32)
                value = pair[(k % 2) * 8 : (k % 2) * 8 + 8]
                shift = bias_p[pl.ds(k, 8, stride=STRIDE), :] + scale
                log2_decay = jnp.tanh(raw[at, lanes]) * scale + shift
                decay = jnp.exp2(log2_decay)
                left = jnp.tanh(log2_decay * -LN2) * (1.0 + decay * decay)
                inlet = raw[at, head + c * LANES : head + (c + 1) * LANES]
                drive = (
                    left * lax.rsqrt(jnp.maximum(left, 1e-37)) * ((1.0 + jnp.tanh(inlet)) * value)
                )
                st = decay * st + drive
                pt = decay * pt
                state[s, c, at, :] = st
                prod[s, c, at, :] = pt
            for d in (1, 2, 4):
                inside = sublane >= d
                st = st + pt * jnp.where(inside, pltpu.roll(st, d, 0), 0.0)
                pt = pt * jnp.where(inside, pltpu.roll(pt, d, 0), 1.0)
            s_in = jnp.where(i == 0, 0.0, carry[2 * c])
            p_in = jnp.where(i == 0, 1.0, carry[2 * c + 1])
            inside = sublane >= 1
            s_ex = jnp.where(inside, pltpu.roll(st, 1, 0), 0.0)
            p_ex = jnp.where(inside, pltpu.roll(pt, 1, 0), 1.0)
            pre_s[s, c] = s_ex + p_ex * s_in
            pre_p[s, c] = p_ex * p_in
            p_last = spread(pt[7:8])
            after += [spread(st[7:8]) + p_last * s_in, p_last * p_in]
        return tuple(after)

    def start_carry():
        zero, one = jnp.zeros((8, LANES), F32), jnp.ones((8, LANES), F32)
        return (zero, one) * parts

    def end_copy(h, d):
        k = h * n_sp + d
        return remote(
            ends.at[h], ends_in.at[k], end_send.at[k], end_recv.at[k],
            {"sp": jnp.minimum(sp + d, n_sp - 1)},
        )

    def send_ends(h, carry):
        for c in range(parts):
            ends[h, c, 0:8, :] = carry[2 * c]
            ends[h, c, 8:16, :] = carry[2 * c + 1]
        for d in range(1, n_sp):
            pl.when(sp + d < n_sp)(end_copy(h, d).start)

    def take_ends(h):
        carry = [jnp.zeros((8, LANES), F32)] * parts
        for d in range(n_sp - 1, 0, -1):
            pl.when(sp >= d)(end_copy(h, d).wait_recv)
            k = h * n_sp + d
            for c in range(parts):
                new = ends_in[k, c, 0:8, :] + ends_in[k, c, 8:16, :] * carry[c]
                carry[c] = jnp.where(d <= sp, new, carry[c])
        return carry

    def a_copy(h, k):
        to = lax.rem(tp + k, n_tp)
        at = pl.ds(pl.multiple_of(to * out_rows, out_rows), out_rows)
        slot = h * n_tp + k
        return remote(
            gated.at[h, at], arrived.at[tp * heads + h], a_send.at[slot], a_recv.at[slot],
            {"tp": to},
        )

    def q_copy(h, k):
        to = lax.rem(tp + k, n_tp)
        slot = h * n_tp + k
        return remote(
            squares.at[h * n_tp + to], squares_in.at[tp * heads + h],
            q_send.at[slot], q_recv.at[slot], {"tp": to},
        )

    def own_copies(h):
        at = pl.ds(pl.multiple_of(tp * out_rows, out_rows), out_rows)
        return (
            pltpu.make_async_copy(gated.at[h, at], arrived.at[tp * heads + h], own_sem.at[2 * h]),
            pltpu.make_async_copy(
                squares.at[h * n_tp + tp], squares_in.at[tp * heads + h], own_sem.at[2 * h + 1]
            ),
        )

    order = list(range(2, n_tp)) + [1, 0]

    def phase_b(h, carry):
        gains = [spread(out_gain[0:1, lanes_of(h, c)]) for c in range(parts)]

        def block(to, j):
            s = h * chunks + to * per_owner + j
            for c in range(parts):
                start = pre_s[s, c] + pre_p[s, c] * carry[c]
                for k in range(SEG):
                    at = slice(k * 8, k * 8 + 8)
                    full = state[s, c, at, :] + prod[s, c, at, :] * start
                    natural[c, pl.ds(k, 8, stride=STRIDE), :] = full * gate[s, c, at, :]
            first = pl.multiple_of(to * out_rows + j * CHUNK, CHUNK)
            sums = []
            for g in range(8):
                part = None
                for c in range(parts):
                    value = natural[c, g * STRIDE : g * STRIDE + SEG, :]
                    gain = jnp.concatenate([gains[c]] * (SEG // 8), axis=0)
                    into = pl.ds(pl.multiple_of(first + g * SEG, SEG), SEG)
                    gated[h, into, c * LANES : (c + 1) * LANES] = (value * gain).astype(BF16)
                    part = value * value if part is None else part + value * value
                sums.append(part)
            row = jnp.sum(jnp.concatenate(sums, axis=0).T, axis=0, keepdims=True)
            at = pl.ds(pl.multiple_of(j * CHUNK, CHUNK), CHUNK)
            squares[h * n_tp + to, :, at] = spread(row)

        def owner(n, _):
            k = lax.rem(n + 2, n_tp)
            k = jnp.where(n == n_tp - 2, 1, jnp.where(n == n_tp - 1, 0, k))
            to = lax.rem(tp + k, n_tp)

            def one(j, _):
                block(to, j)
                return 0

            lax.fori_loop(0, per_owner, one, 0)

            @pl.when(k == 0)
            def _():
                for copy in own_copies(h):
                    copy.start()

            @pl.when(k > 0)
            def _():
                a_copy(h, k).start()
                q_copy(h, k).start()

            return 0

        lax.fori_loop(0, n_tp, owner, 0)

    h_all = range(heads)
    for h in h_all:
        gates_w[h, :, 0:head] = w_rate[h] * 0.5
        gates_w[h, :, head : 2 * head] = w_inlet[h] * 0.5
    scale_row[...] = softplus_of_minus(decay_param[...]) * (-4.0 / LN2)
    fold(0)
    x_copy(0).wait()
    x_copy(1).start()
    for h in range(1, heads):
        for copy in w_copies(h):
            copy.start()
    acc, scale = project(0, True)
    for c in range(parts):
        proj[c, 7 * STRIDE + SEG : 8 * STRIDE, :] = jnp.zeros((8, LANES), F32)

    pl.semaphore_wait(barrier, n_sp - 1 + n_tp - 1 + 1)
    pl.when(sp < n_sp - 1)(halo_copy.start)
    for p in range(pieces):
        pl.when(sp < n_sp - 1)(own_copy(True, p).start)
        pl.when(sp > 0)(own_copy(False, p).start)
    for h in range(1, heads):
        fold(h)
    for i in range(2, chunks):
        x_copy(i).start()
    out_load.start()

    @pl.when(sp == 0)
    def _():
        before[...] = jnp.zeros_like(before)

    @pl.when(sp > 0)
    def _():
        halo_copy.wait_recv()
        halo_inv = norm_of(halo[...])
        for h in h_all:
            rows_before = jnp.dot(halo[...], w_in[h, :, 0:head], preferred_element_type=F32)
            rows_before = rows_before * halo_inv
            for c in range(parts):
                before[h, c] = rows_before[halo_rows - 8 :, c * LANES : (c + 1) * LANES]

    keep(0, acc, scale)
    x_copy(1).wait()
    acc, scale = project(1, True)
    convolve(0)
    keep(1, acc, scale)

    def finish_step(s, carry):
        @pl.when(s % chunks == chunks - 1)
        def _():
            send_ends(s // chunks, carry)

    def step(sums, s, carry):
        if sums:
            x_copy(s + 2).wait()

        @pl.when((s >= FIRST) & ((s - FIRST) % EVERY == 0))
        def _():
            pump((s - FIRST) // EVERY)

        if not sums and heads > 1:

            @pl.when((s >= chunks) & (s % chunks == BEHIND))
            def _():
                phase_b(s // chunks - 1, take_ends(s // chunks - 1))

        acc, scale = project(s + 2, sums)
        carry = elementwise(s, carry)
        convolve(s + 1)
        keep(s + 2, acc, scale)
        finish_step(s, carry)
        return carry

    carry = start_carry()
    carry = lax.fori_loop(0, chunks - 2, functools.partial(step, True), carry)
    carry = lax.fori_loop(chunks - 2, steps - 2, functools.partial(step, False), carry)
    done = -((FIRST - steps + 2) // EVERY)
    carry = elementwise(steps - 2, carry)
    convolve(steps - 1)
    carry = elementwise(steps - 1, carry)
    last = heads - 1
    send_ends(last, carry)
    pump(done)
    done += 1

    def pump_some(first, end):
        def one(n, _):
            pump(n)
            return 0

        lax.fori_loop(first, end, one, 0)

    phase_b(last, take_ends(last))
    out_load.wait()

    progressive = shard == channels
    tile = 512 if width % 512 == 0 else 256
    deep = min(shard, head)

    def wait_from(k, h):
        @pl.when(k == 0)
        def _():
            for copy in own_copies(h):
                copy.wait()

        @pl.when(k > 0)
        def _():
            a_copy(h, k).wait_recv()
            q_copy(h, k).wait_recv()

    def wait_mate(b):
        source = source_of(b)

        def one(p, _):
            m_copy(source, p, False, True).wait_recv()
            m_copy(source, p, True, True).wait_recv()
            return 0

        lax.fori_loop(0, pieces, one, 0)

    def prepare(b, h):
        source = source_of(b)
        if progressive:
            wait_from(lax.rem(tp - source + n_tp, n_tp), h)
        return source

    def multiply(source, columns, units):
        blocks = []
        for u in units:
            at = source * shard + u * deep
            from_col = pl.multiple_of(at % head, deep)
            blocks.append(arrived[at // head, :, pl.ds(from_col, deep)])
        left = jnp.concatenate(blocks, axis=1)
        first = pl.multiple_of(source * shard + units[0] * deep, deep)
        right = w_all[pl.ds(first, len(units) * deep), columns]
        return jnp.dot(left, right, preferred_element_type=F32)

    def columns_at(n):
        return pl.ds(pl.multiple_of(n * tile, tile), tile)

    if not progressive:
        for k in range(n_tp):
            for h in h_all:
                wait_from(k, h)
    units = shard // deep
    work = [(b, u) for u in range(units) for b in range(n_sp - 1)]
    ahead = max(done, AHEAD * items // 12)
    pump_some(done, ahead)
    cursor = ahead
    mates = {0}
    for index, (b, u) in enumerate(work):
        needed = b * pieces + LAG
        if index >= n_sp - 1 and progressive:
            needed = items + LAG
        if b > 0:
            pump_some(cursor, max(cursor, needed))
            cursor = max(cursor, needed)
        if b not in mates:
            wait_mate(b)
            mates.add(b)
        source = prepare(b, u)

        def partial_sum(n, _, source=source, index=index, u=u, cursor=cursor):
            columns = columns_at(n)
            value = multiply(source, columns, (u,))
            total[:, columns] = value if index == 0 else total[:, columns] + value

            @pl.when((n < BETWEEN) & (cursor + n < items + LAG))
            def _():
                pump(cursor + n)

            return 0

        lax.fori_loop(0, width // tile, partial_sum, 0)
        cursor = min(cursor + BETWEEN, items + LAG)
    b = n_sp - 1
    if b > 0:
        pump_some(cursor, items + LAG)
        wait_mate(b)
    for u in range(units):
        source = prepare(b, u)
    row = squares_in[0]
    for k in range(1, n_tp * heads):
        row = row + squares_in[k]
    out_scale = lax.rsqrt(row[0:1] / (n_tp * heads * head) + 1e-06)
    scale_cols = jnp.broadcast_to(out_scale, (LANES, out_rows)).T

    def out_copy(n):
        columns = columns_at(n)
        return pltpu.make_async_copy(result.at[:, columns], out.at[:, columns], out_sem.at[n])

    def final(n, _):
        columns = columns_at(n)
        value = multiply(source, columns, tuple(range(units)))
        if n_sp > 1:
            value = value + total[:, columns]
        value = value * jnp.concatenate([scale_cols] * (tile // LANES), axis=1)
        result[:, columns] = value.astype(BF16)
        out_copy(n).start()
        return 0

    lax.fori_loop(0, width // tile, final, 0)

    pl.when(sp < n_sp - 1)(halo_copy.wait_send)
    for p in range(pieces):
        pl.when(sp < n_sp - 1)(own_copy(True, p).wait_send)
        pl.when(sp > 0)(own_copy(False, p).wait_send)

    def drain_one(source, p, from_left):
        onward(source, p, from_left, lambda copy: copy.wait_send())
        y_copy(source, p).wait_send()
        m_copy(source, p, False).wait_send()
        m_copy(source, p, True).wait_send()

    def drain(n, _):
        each_source(n, drain_one)
        return 0

    lax.fori_loop(0, items, drain, 0)
    for h in h_all:
        for d in range(1, n_sp):
            pl.when(sp + d < n_sp)(end_copy(h, d).wait_send)
        for k in range(1, n_tp):
            a_copy(h, k).wait_send()
            q_copy(h, k).wait_send()
    for n in range(width // tile):
        out_copy(n).wait()


def body(sizes, tokens, in_gain, w_input, w_gate, conv_taps, w_rate, w_inlet, decay_param,
         decay_bias, out_gain, w_out):
    n_grp, n_sp, n_tp = sizes
    rows, width = tokens.shape
    channels = w_input.shape[1]
    heads, head = w_rate.shape[0], w_rate.shape[1]
    parts = head // LANES
    steps = heads * (rows // CHUNK)
    out_rows = rows // n_tp
    out_width = w_out.shape[1]
    shard = w_out.shape[0]
    quarter = shard // (2 * n_grp)
    pieces = quarter // max(16, quarter // 4)
    all_channels = channels * n_tp
    tile = 512 if out_width % 512 == 0 else 256
    hbm = pl.BlockSpec(memory_space=pl.ANY)
    vmem = pl.BlockSpec(memory_space=pltpu.VMEM)
    dma = pltpu.SemaphoreType.DMA
    return pl.pallas_call(
        functools.partial(kernel, sizes),
        out_shape=jax.ShapeDtypeStruct((out_rows, out_width), BF16),
        in_specs=[hbm, vmem, hbm, hbm, vmem, vmem, vmem, vmem, vmem, vmem, hbm],
        out_specs=hbm,
        scratch_shapes=[
            pltpu.VMEM((rows, width), BF16),
            pltpu.VMEM((heads, width, 2 * head), BF16),
            pltpu.VMEM((all_channels, out_width), BF16),
            pltpu.VMEM((heads, head, 2 * head), BF16),
            pltpu.VMEM((rows, LANES), F32),
            pltpu.VMEM((parts, 8 * STRIDE, LANES), F32),
            pltpu.VMEM((parts, 8 * STRIDE, LANES), F32),
            pltpu.VMEM((CHUNK, head), BF16),
            pltpu.VMEM((CHUNK, 2 * head), F32),
            pltpu.VMEM((8 * STRIDE, LANES), F32),
            pltpu.VMEM((1, channels), F32),
            pltpu.VMEM((heads, parts, 8, LANES), F32),
            pltpu.VMEM((steps, parts, CHUNK, LANES), F32),
            pltpu.VMEM((steps, parts, CHUNK, LANES), F32),
            pltpu.VMEM((steps, parts, CHUNK, LANES), F32),
            pltpu.VMEM((steps, parts, 8, LANES), F32),
            pltpu.VMEM((steps, parts, 8, LANES), F32),
            pltpu.VMEM((parts, 8 * STRIDE, LANES), F32),
            pltpu.VMEM((heads, rows, head), BF16),
            pltpu.VMEM((n_tp * heads, out_rows, head), BF16),
            pltpu.VMEM((out_rows, out_width), F32),
            pltpu.VMEM((out_rows, out_width), BF16),
            pltpu.VMEM((16, width), BF16),
            pltpu.VMEM((heads * n_tp, 8, out_rows), F32),
            pltpu.VMEM((n_tp * heads, 8, out_rows), F32),
            pltpu.VMEM((heads, parts, 16, LANES), F32),
            pltpu.VMEM((heads * n_sp, parts, 16, LANES), F32),
            dma((rows // CHUNK,)),
            dma((2 * heads,)),
            dma,
            dma,
            dma,
            dma((2 * n_sp * pieces,)),
            dma((n_sp * pieces,)),
            dma((n_sp * pieces,)),
            dma((n_sp * pieces,)),
            dma((2 * n_sp * pieces,)),
            dma((2 * n_sp * pieces,)),
            dma((heads * n_sp,)),
            dma((heads * n_sp,)),
            dma((heads * n_tp,)),
            dma((heads * n_tp,)),
            dma((heads * n_tp,)),
            dma((heads * n_tp,)),
            dma((2 * heads,)),
            dma((out_width // tile,)),
        ],
        compiler_params=pltpu.CompilerParams(
            collective_id=0, has_side_effects=True, vmem_limit_bytes=62 * 1024 * 1024
        ),
    )(
        tokens, in_gain.reshape(1, width), w_input, w_gate, conv_taps, w_rate, w_inlet,
        decay_param.reshape(1, channels), decay_bias, out_gain.reshape(1, channels), w_out,
    )


def solution(mesh):
    sizes = (mesh.shape["grp"], mesh.shape["sp"], mesh.shape["tp"])
    return jax.shard_map(
        functools.partial(body, sizes),
        mesh=mesh,
        in_specs=(
            P(("grp", "sp"), None),
            P(),
            P(None, "tp"),
            P(None, "tp"),
            P(None, "tp"),
            P("tp", None, None),
            P("tp", None, None),
            P("tp"),
            P("tp", ("grp", "sp")),
            P("tp"),
            P("sp", None),
        ),
        out_specs=P(("grp", "sp", "tp"), None),
        check_vma=False,
    )
```

```python
import functools
import math
import jax
import jax.numpy as jnp
from jax import lax
from jax.experimental import pallas as pl
from jax.experimental.pallas import tpu as pltpu
from jax.sharding import PartitionSpec as P

MESH = pl.DeviceIdType.MESH
F32 = jnp.float32
BF16 = jnp.bfloat16
CHUNK = 256
SEG = CHUNK // 8
STRIDE = SEG + 8
LANES = 128
LAG = 6
FIRST = 1
EVERY = 3
BEHIND = 3
AHEAD = 7
EARLY = 3
BETWEEN = 1
REST = 4
LN2 = math.log(2.0)
GELU_A = math.sqrt(2.0 / math.pi)
GELU_B = GELU_A * 0.044715


def gelu_half(value):
    inner = value * (GELU_A + GELU_B * (value * value))
    return (0.25 * value) * (1.0 + jnp.tanh(inner))


def softplus_of_minus(value):
    small = jnp.exp(-jnp.abs(value))
    z = small / (2.0 + small)
    zz = z * z
    series = 1.0 / 15.0
    for n in (13, 11, 9, 7, 5, 3, 1):
        series = series * zz + 1.0 / n
    return jnp.maximum(-value, 0.0) + 2.0 * z * series


def spread(row):
    return jnp.broadcast_to(row, (8, row.shape[1]))


def columns_of(row):
    return jnp.broadcast_to(row, (LANES, row.shape[1])).T


def kernel(
    sizes,
    tokens, in_gain_h, w_input, w_gate, taps_h, w_rate, w_inlet, decay_h, bias_h, out_gain_h, w_out,
    out,
    in_gain, taps, decay_param, bias, out_gain, tail,
    x, w_in, w_all, gates_w, inv, proj, graw, conv, raw, bias_p, scale_row, before,
    state, prod, gate, pre_s, pre_p, natural, gated, arrived, total, result, halo,
    squares, squares_in, ends, ends_in,
    x_sem, w_sem, out_load_sem, halo_send, halo_recv, z_send, z_recv, y_send, y_recv,
    m_send, m_recv, end_send, end_recv, a_send, a_recv, q_send, q_recv, own_sem, out_sem,
    small_sem, tail_sem,
):
    n_grp, n_sp, n_tp = sizes
    grp, sp, tp = lax.axis_index("grp"), lax.axis_index("sp"), lax.axis_index("tp")
    rows, width = tokens.shape
    heads, head = w_rate.shape[0], w_rate.shape[1]
    parts = head // LANES
    channels = heads * head
    reach = taps.shape[0] - 1
    chunks = rows // CHUNK
    steps = heads * chunks
    out_rows = rows // n_tp
    per_owner = out_rows // CHUNK
    shard = w_out.shape[0]
    quarter = shard // (2 * n_grp)
    piece = max(16, quarter // 4)
    pieces = quarter // piece
    items = (n_sp - 1) * pieces
    core = lax.rem(tp, 2)
    mate = tp + 1 - 2 * core
    across = 1 - grp

    def x_copy(i):
        at = pl.ds(pl.multiple_of(i * CHUNK, CHUNK), CHUNK)
        return pltpu.make_async_copy(tokens.at[at], x.at[at], x_sem.at[i])

    def w_copies(h):
        lanes = pl.ds(h * head, head)
        return (
            pltpu.make_async_copy(w_input.at[:, lanes], w_in.at[h, :, 0:head], w_sem.at[2 * h]),
            pltpu.make_async_copy(
                w_gate.at[:, lanes], w_in.at[h, :, head : 2 * head], w_sem.at[2 * h + 1]
            ),
        )

    out_load = pltpu.make_async_copy(
        w_out, w_all.at[pl.ds(pl.multiple_of(sp * shard, shard), shard)], out_load_sem
    )

    smalls = [
        pltpu.make_async_copy(source, target, small_sem.at[n])
        for n, (source, target) in enumerate((
            (in_gain_h, in_gain), (w_rate, gates_w.at[:, :, 0:head]),
            (w_inlet, gates_w.at[:, :, head : 2 * head]), (decay_h, decay_param),
            (bias_h, bias), (taps_h, taps), (out_gain_h, out_gain),
        ))
    ]
    ends_in[...] = jnp.zeros_like(ends_in)
    barrier = pltpu.get_barrier_semaphore()
    for d in range(1, n_sp):
        pl.semaphore_signal(
            barrier, inc=1, device_id={"sp": lax.rem(sp + d, n_sp)}, device_id_type=MESH
        )
    for k in range(1, n_tp):
        pl.semaphore_signal(
            barrier, inc=1, device_id={"tp": lax.rem(tp + k, n_tp)}, device_id_type=MESH
        )
    pl.semaphore_signal(barrier, inc=1, device_id={"grp": across}, device_id_type=MESH)

    smalls[0].start()
    for copy in w_copies(0):
        copy.start()
    halo_rows = halo.shape[0]
    tail_copy = pltpu.make_async_copy(
        tokens.at[pl.ds(rows - halo_rows, halo_rows)], tail, tail_sem
    )
    tail_copy.start()
    x_copy(0).start()
    for copy in smalls[1:]:
        copy.start()

    def remote(src, dst, send, recv, where):
        return pltpu.make_async_remote_copy(
            src_ref=src, dst_ref=dst, send_sem=send, recv_sem=recv,
            device_id=where, device_id_type=MESH,
        )

    halo_copy = remote(
        tail, halo, halo_send, halo_recv,
        {"sp": jnp.minimum(sp + 1, n_sp - 1)},
    )

    def w_rows(source, which, p):
        first = source * shard + which * quarter + p * piece
        return w_all.at[pl.ds(pl.multiple_of(first, piece), piece)]

    def which_of(other, owner):
        return (across if other else grp) * 2 + owner

    def own_copy(to_right, p):
        mine = which_of(False, core)
        first = pl.multiple_of(mine * quarter + p * piece, piece)
        slot = ((0 if to_right else 1) * n_sp + sp) * pieces + p
        return remote(
            w_out.at[pl.ds(first, piece)], w_rows(sp, mine, p),
            z_send.at[slot], z_recv.at[sp * pieces + p],
            {"sp": jnp.minimum(sp + 1, n_sp - 1) if to_right else jnp.maximum(sp - 1, 0)},
        )

    def z_copy(source, p, to_right):
        at = w_rows(source, which_of(False, core), p)
        slot = ((0 if to_right else 1) * n_sp + source) * pieces + p
        return remote(
            at, at, z_send.at[slot], z_recv.at[source * pieces + p],
            {"sp": jnp.minimum(sp + 1, n_sp - 1) if to_right else jnp.maximum(sp - 1, 0)},
        )

    def y_copy(source, p, incoming=False):
        at = w_rows(source, which_of(incoming, core), p)
        slot = source * pieces + p
        return remote(at, at, y_send.at[slot], y_recv.at[slot], {"grp": across})

    def m_copy(source, p, second, incoming=False):
        at = w_rows(source, which_of(second, 1 - core if incoming else core), p)
        slot = ((1 if second else 0) * n_sp + source) * pieces + p
        return remote(at, at, m_send.at[slot], m_recv.at[slot], {"tp": mate})

    inner = jnp.minimum(sp, n_sp - 1 - sp)
    leftward = sp > n_sp - 1 - sp

    def source_of(b):
        d = jnp.where(b <= 2 * inner, (b + 1) // 2, b - inner)
        from_left = jnp.where(b <= 2 * inner, b % 2 == 1, leftward)
        return jnp.where(from_left, sp - d, sp + d)

    held = (1, 2) if heads > 1 else ()

    def each_source(n, action):
        d, p = 1 + n // pieces, n % pieces

        @pl.when(sp >= d)
        def _():
            action(sp - d, p, True)

        @pl.when(sp + d < n_sp)
        def _():
            action(sp + d, p, False)

    def onward(source, p, from_left, act):
        if from_left:
            pl.when(sp < n_sp - 1)(lambda: act(z_copy(source, p, True)))
        else:
            pl.when(sp > 0)(lambda: act(z_copy(source, p, False)))

    def take_z(source, p, from_left):
        z_copy(source, p, from_left).wait_recv()
        y_copy(source, p).start()
        m_copy(source, p, False).start()

    def take_y(source, p, from_left):
        y_copy(source, p, True).wait_recv()
        m_copy(source, p, True).start()

    def send_on(up, source, p, from_left):
        if up == from_left:
            onward(source, p, from_left, lambda copy: copy.start())

    def pump(n):
        @pl.when(n < items)
        def _():
            each_source(n, take_z)
            each_source(n, functools.partial(send_on, False))

        @pl.when(((n < min(held, default=0)) | (n > max(held, default=-1))) & (n < items))
        def _():
            each_source(n, functools.partial(send_on, True))

        @pl.when(n >= LAG)
        def _():
            each_source(n - LAG, take_y)

    def fold(h):
        def block(j, _):
            at = pl.ds(pl.multiple_of(j * CHUNK, CHUNK), CHUNK)
            gain = columns_of(in_gain[0:1, at])
            for c in range(2 * parts):
                lanes = slice(c * LANES, (c + 1) * LANES)
                w_in[h, at, lanes] = (w_in[h, at, lanes].astype(F32) * gain).astype(BF16)
            return 0

        lax.fori_loop(0, width // CHUNK, block, 0)

    def norm_of(chunk):
        as_float = chunk.astype(F32)
        return lax.rsqrt(jnp.mean(as_float * as_float, axis=1, keepdims=True) + 1e-06)

    def lanes_of(h, c):
        return pl.ds(pl.multiple_of(h * head + c * LANES, LANES), LANES)

    def project(s, sums):
        h, i = s // chunks, s % chunks
        at = pl.ds(pl.multiple_of(i * CHUNK, CHUNK), CHUNK)
        acc = jnp.dot(x[at, :], w_in[h], preferred_element_type=F32)
        if sums:
            scale = jnp.broadcast_to(norm_of(x[at, :]), (CHUNK, LANES))
            inv[at, :] = scale
        else:
            scale = inv[at, :]
        return acc, scale

    def keep(s, acc, scale):
        h, i = s // chunks, s % chunks
        for c in range(parts):
            last = proj[c, 7 * STRIDE + SEG : 8 * STRIDE, :]
            proj[c, 0:8, :] = jnp.where(i == 0, before[h, c], last)
            for g in range(8):
                at = slice(g * SEG, (g + 1) * SEG)
                block = acc[at, c * LANES : (c + 1) * LANES] * scale[at]
                proj[c, g * STRIDE + 8 : (g + 1) * STRIDE, :] = block
                if g < 7:
                    proj[c, (g + 1) * STRIDE : (g + 1) * STRIDE + 8, :] = block[SEG - 8 :]
                other = acc[at, head + c * LANES : head + (c + 1) * LANES] * scale[at]
                graw[c, g * STRIDE : g * STRIDE + SEG, :] = other

    def convolve(s):
        h, i = s // chunks, s % chunks
        for c in range(parts):
            lanes = lanes_of(h, c)
            tap = [spread(taps[k : k + 1, lanes]) for k in range(reach + 1)]
            window = [
                proj[c, pl.ds(8 - reach + j, 8, stride=STRIDE), :] for j in range(SEG + reach)
            ]
            done = []
            for k in range(SEG):
                summed = window[k] * tap[0]
                for j in range(1, reach + 1):
                    summed = summed + window[k + j] * tap[j]
                done.append(summed)
            for k in range(SEG):
                value = graw[c, pl.ds(k, 8, stride=STRIDE), :]
                gate[s, c, k * 8 : k * 8 + 8, :] = gelu_half(value)
            for k in range(0, SEG, 2):
                pair = jnp.concatenate(done[k : k + 2], axis=0).astype(BF16)
                conv[k * 8 : k * 8 + 16, c * LANES : (c + 1) * LANES] = pair
        row = bias[pl.ds(h, 1), pl.ds(pl.multiple_of(i * CHUNK, CHUNK), CHUNK)] * (1.0 / LN2)
        cols = columns_of(row)
        for g in range(8):
            bias_p[g * STRIDE : g * STRIDE + SEG, :] = cols[g * SEG : (g + 1) * SEG]
        raw[...] = jnp.dot(conv[...], gates_w[h], preferred_element_type=F32)

    sublane = lax.broadcasted_iota(jnp.int32, (8, LANES), 0)

    def elementwise(s, carry):
        h, i = s // chunks, s % chunks
        after = []
        for c in range(parts):
            scale = spread(scale_row[0:1, lanes_of(h, c)])
            lanes = slice(c * LANES, (c + 1) * LANES)
            st, pt = jnp.zeros((8, LANES), F32), jnp.ones((8, LANES), F32)
            for k in range(SEG):
                at = slice(k * 8, k * 8 + 8)
                if k % 2 == 0:
                    pair = conv[k * 8 : k * 8 + 16, lanes].astype(F32)
                value = pair[(k % 2) * 8 : (k % 2) * 8 + 8]
                shift = bias_p[pl.ds(k, 8, stride=STRIDE), :] + scale
                log2_decay = jnp.tanh(raw[at, lanes]) * scale + shift
                decay = jnp.exp2(log2_decay)
                left = jnp.tanh(log2_decay * -LN2) * (1.0 + decay * decay)
                inlet = raw[at, head + c * LANES : head + (c + 1) * LANES]
                drive = (
                    left * lax.rsqrt(jnp.maximum(left, 1e-37)) * ((1.0 + jnp.tanh(inlet)) * value)
                )
                st = decay * st + drive
                pt = decay * pt
                state[s, c, at, :] = st
                prod[s, c, at, :] = pt
            for d in (1, 2, 4):
                inside = sublane >= d
                st = st + pt * jnp.where(inside, pltpu.roll(st, d, 0), 0.0)
                pt = pt * jnp.where(inside, pltpu.roll(pt, d, 0), 1.0)
            s_in = jnp.where(i == 0, 0.0, carry[2 * c])
            p_in = jnp.where(i == 0, 1.0, carry[2 * c + 1])
            inside = sublane >= 1
            s_ex = jnp.where(inside, pltpu.roll(st, 1, 0), 0.0)
            p_ex = jnp.where(inside, pltpu.roll(pt, 1, 0), 1.0)
            pre_s[s, c] = s_ex + p_ex * s_in
            pre_p[s, c] = p_ex * p_in
            p_last = spread(pt[7:8])
            after += [spread(st[7:8]) + p_last * s_in, p_last * p_in]
        return tuple(after)

    def start_carry():
        zero, one = jnp.zeros((8, LANES), F32), jnp.ones((8, LANES), F32)
        return (zero, one) * parts

    def end_copy(h, d):
        k = h * n_sp + d
        return remote(
            ends.at[h], ends_in.at[k], end_send.at[k], end_recv.at[k],
            {"sp": jnp.minimum(sp + d, n_sp - 1)},
        )

    def send_ends(h, carry):
        for c in range(parts):
            ends[h, c, 0:8, :] = carry[2 * c]
            ends[h, c, 8:16, :] = carry[2 * c + 1]
        for d in range(1, n_sp):
            pl.when(sp + d < n_sp)(end_copy(h, d).start)

    def take_ends(h):
        carry = [jnp.zeros((8, LANES), F32)] * parts
        for d in range(n_sp - 1, 0, -1):
            pl.when(sp >= d)(end_copy(h, d).wait_recv)
            k = h * n_sp + d
            for c in range(parts):
                new = ends_in[k, c, 0:8, :] + ends_in[k, c, 8:16, :] * carry[c]
                carry[c] = jnp.where(d <= sp, new, carry[c])
        return carry

    def a_copy(h, k):
        to = lax.rem(tp + k, n_tp)
        at = pl.ds(pl.multiple_of(to * out_rows, out_rows), out_rows)
        slot = h * n_tp + k
        return remote(
            gated.at[h, at], arrived.at[tp * heads + h], a_send.at[slot], a_recv.at[slot],
            {"tp": to},
        )

    def q_copy(h, k):
        to = lax.rem(tp + k, n_tp)
        slot = h * n_tp + k
        return remote(
            squares.at[h * n_tp + to], squares_in.at[tp * heads + h],
            q_send.at[slot], q_recv.at[slot], {"tp": to},
        )

    def own_copies(h):
        at = pl.ds(pl.multiple_of(tp * out_rows, out_rows), out_rows)
        return (
            pltpu.make_async_copy(gated.at[h, at], arrived.at[tp * heads + h], own_sem.at[2 * h]),
            pltpu.make_async_copy(
                squares.at[h * n_tp + tp], squares_in.at[tp * heads + h], own_sem.at[2 * h + 1]
            ),
        )

    order = list(range(2, n_tp)) + [1, 0]

    def phase_b(h, carry):
        gains = [spread(out_gain[0:1, lanes_of(h, c)]) for c in range(parts)]

        def block(to, j):
            s = h * chunks + to * per_owner + j
            for c in range(parts):
                start = pre_s[s, c] + pre_p[s, c] * carry[c]
                for k in range(SEG):
                    at = slice(k * 8, k * 8 + 8)
                    full = state[s, c, at, :] + prod[s, c, at, :] * start
                    natural[c, pl.ds(k, 8, stride=STRIDE), :] = full * gate[s, c, at, :]
            first = pl.multiple_of(to * out_rows + j * CHUNK, CHUNK)
            sums = []
            for g in range(8):
                part = None
                for c in range(parts):
                    value = natural[c, g * STRIDE : g * STRIDE + SEG, :]
                    gain = jnp.concatenate([gains[c]] * (SEG // 8), axis=0)
                    into = pl.ds(pl.multiple_of(first + g * SEG, SEG), SEG)
                    gated[h, into, c * LANES : (c + 1) * LANES] = (value * gain).astype(BF16)
                    part = value * value if part is None else part + value * value
                sums.append(part)
            row = jnp.sum(jnp.concatenate(sums, axis=0).T, axis=0, keepdims=True)
            at = pl.ds(pl.multiple_of(j * CHUNK, CHUNK), CHUNK)
            squares[h * n_tp + to, :, at] = spread(row)

        def owner(n, _):
            k = lax.rem(n + 2, n_tp)
            k = jnp.where(n == n_tp - 2, 1, jnp.where(n == n_tp - 1, 0, k))
            to = lax.rem(tp + k, n_tp)

            def one(j, _):
                block(to, j)
                return 0

            lax.fori_loop(0, per_owner, one, 0)

            @pl.when(k == 0)
            def _():
                for copy in own_copies(h):
                    copy.start()

            @pl.when(k > 0)
            def _():
                a_copy(h, k).start()
                q_copy(h, k).start()

            return 0

        lax.fori_loop(0, n_tp, owner, 0)

    h_all = range(heads)
    smalls[0].wait()
    for copy in w_copies(0):
        copy.wait()
    for h in range(1, heads):
        for copy in w_copies(h):
            copy.start()
    x_copy(1).start()
    fold(0)
    tail_copy.wait()
    pl.semaphore_wait(barrier, n_sp - 1 + n_tp - 1 + 1)
    pl.when(sp < n_sp - 1)(halo_copy.start)
    for p in range(pieces):
        pl.when(sp < n_sp - 1)(own_copy(True, p).start)
        pl.when(sp > 0)(own_copy(False, p).start)
    x_copy(0).wait()
    acc, scale = project(0, True)
    for c in range(parts):
        proj[c, 7 * STRIDE + SEG : 8 * STRIDE, :] = jnp.zeros((8, LANES), F32)
    for copy in smalls[1:]:
        copy.wait()
    for h in h_all:
        gates_w[h] = gates_w[h] * 0.5
    scale_row[...] = softplus_of_minus(decay_param[...]) * (-4.0 / LN2)
    for h in range(1, heads):
        for copy in w_copies(h):
            copy.wait()
        fold(h)
    for i in range(2, chunks):
        x_copy(i).start()
    out_load.start()

    @pl.when(sp == 0)
    def _():
        before[...] = jnp.zeros_like(before)

    @pl.when(sp > 0)
    def _():
        halo_copy.wait_recv()
        halo_inv = norm_of(halo[...])
        for h in h_all:
            rows_before = jnp.dot(halo[...], w_in[h, :, 0:head], preferred_element_type=F32)
            rows_before = rows_before * halo_inv
            for c in range(parts):
                before[h, c] = rows_before[halo_rows - 8 :, c * LANES : (c + 1) * LANES]

    keep(0, acc, scale)
    x_copy(1).wait()
    acc, scale = project(1, True)
    convolve(0)
    keep(1, acc, scale)

    def finish_step(s, carry):
        @pl.when(s % chunks == chunks - 1)
        def _():
            send_ends(s // chunks, carry)

    def step(sums, s, carry):
        if sums:
            x_copy(s + 2).wait()

        if not sums and heads > 1:

            @pl.when(s == chunks)
            def _():
                for k in held:
                    each_source(k, functools.partial(send_on, True))

        @pl.when((s >= FIRST) & ((s - FIRST) % EVERY == 0))
        def _():
            pump((s - FIRST) // EVERY)

        if not sums and heads > 1:

            @pl.when((s >= chunks) & (s % chunks == BEHIND))
            def _():
                phase_b(s // chunks - 1, take_ends(s // chunks - 1))

        acc, scale = project(s + 2, sums)
        carry = elementwise(s, carry)
        convolve(s + 1)
        keep(s + 2, acc, scale)
        finish_step(s, carry)
        return carry

    carry = start_carry()
    carry = lax.fori_loop(0, chunks - 2, functools.partial(step, True), carry)
    carry = lax.fori_loop(chunks - 2, steps - 2, functools.partial(step, False), carry)
    done = -((FIRST - steps + 2) // EVERY)
    carry = elementwise(steps - 2, carry)
    convolve(steps - 1)
    carry = elementwise(steps - 1, carry)
    last = heads - 1
    send_ends(last, carry)
    before_last = min(done + EARLY, items + LAG)

    def pump_some(first, end):
        def one(n, _):
            pump(n)
            return 0

        lax.fori_loop(first, end, one, 0)

    pump_some(done, before_last)
    done = before_last
    phase_b(last, take_ends(last))
    out_load.wait()

    progressive = shard == channels
    tile = 512 if width % 512 == 0 else 256
    deep = min(shard, head)

    def wait_from(k, h):
        @pl.when(k == 0)
        def _():
            for copy in own_copies(h):
                copy.wait()

        @pl.when(k > 0)
        def _():
            a_copy(h, k).wait_recv()
            q_copy(h, k).wait_recv()

    def wait_mate(b):
        source = source_of(b)

        def one(p, _):
            m_copy(source, p, False, True).wait_recv()
            m_copy(source, p, True, True).wait_recv()
            return 0

        lax.fori_loop(0, pieces, one, 0)

    def prepare(b, h):
        source = source_of(b)
        if progressive:
            wait_from(lax.rem(tp - source + n_tp, n_tp), h)
        return source

    def multiply(source, columns, units):
        blocks = []
        for u in units:
            at = source * shard + u * deep
            from_col = pl.multiple_of(at % head, deep)
            blocks.append(arrived[at // head, :, pl.ds(from_col, deep)])
        left = jnp.concatenate(blocks, axis=1)
        first = pl.multiple_of(source * shard + units[0] * deep, deep)
        right = w_all[pl.ds(first, len(units) * deep), columns]
        return jnp.dot(left, right, preferred_element_type=F32)

    def columns_at(n):
        return pl.ds(pl.multiple_of(n * tile, tile), tile)

    if not progressive:
        for k in range(n_tp):
            for h in h_all:
                wait_from(k, h)
    units = shard // deep
    work = [(b, u) for u in range(units) for b in range(n_sp - 1)]
    ahead = max(done, AHEAD * items // 12)
    pump_some(done, ahead)
    cursor = ahead
    mates = {0}
    for index, (b, u) in enumerate(work):
        needed = b * pieces + LAG
        if index == n_sp - 1 and progressive:
            needed = max(needed, items + LAG - REST)
        if b > 0:
            pump_some(cursor, max(cursor, needed))
            cursor = max(cursor, needed)
        elif index > 0:
            pump_some(cursor, max(cursor, needed))
            cursor = max(cursor, needed)
        if b not in mates:
            wait_mate(b)
            mates.add(b)
        source = prepare(b, u)

        def partial_sum(n, _, source=source, index=index, u=u, cursor=cursor):
            columns = columns_at(n)
            value = multiply(source, columns, (u,))
            total[:, columns] = value if index == 0 else total[:, columns] + value

            @pl.when((n < BETWEEN) & (cursor + n < items + LAG))
            def _():
                pump(cursor + n)

            return 0

        lax.fori_loop(0, width // tile, partial_sum, 0)
        cursor = min(cursor + BETWEEN, items + LAG)
    def drain_one(source, p, from_left):
        onward(source, p, from_left, lambda copy: copy.wait_send())
        y_copy(source, p).wait_send()
        m_copy(source, p, False).wait_send()
        m_copy(source, p, True).wait_send()

    def drain(n, _):
        each_source(n, drain_one)
        return 0

    drained = max(0, items + LAG - REST - LAG - 2)
    pl.when(sp < n_sp - 1)(halo_copy.wait_send)
    for p in range(pieces):
        pl.when(sp < n_sp - 1)(own_copy(True, p).wait_send)
        pl.when(sp > 0)(own_copy(False, p).wait_send)

    for h in h_all:
        for d in range(1, n_sp):
            pl.when(sp + d < n_sp)(end_copy(h, d).wait_send)
        for k in range(1, n_tp):
            a_copy(h, k).wait_send()
            q_copy(h, k).wait_send()
    lax.fori_loop(0, drained, drain, 0)
    b = n_sp - 1
    if b > 0:
        pump_some(cursor, items + LAG)
        wait_mate(b)
    for u in range(units):
        source = prepare(b, u)
    row = squares_in[0]
    for k in range(1, n_tp * heads):
        row = row + squares_in[k]
    out_scale = lax.rsqrt(row[0:1] / (n_tp * heads * head) + 1e-06)
    scale_cols = jnp.broadcast_to(out_scale, (LANES, out_rows)).T

    def out_copy(n):
        columns = columns_at(n)
        return pltpu.make_async_copy(result.at[:, columns], out.at[:, columns], out_sem.at[n])

    def final(n, _):
        columns = columns_at(n)
        value = multiply(source, columns, tuple(range(units)))
        if n_sp > 1:
            value = value + total[:, columns]
        value = value * jnp.concatenate([scale_cols] * (tile // LANES), axis=1)
        result[:, columns] = value.astype(BF16)
        out_copy(n).start()
        return 0

    lax.fori_loop(0, width // tile, final, 0)

    lax.fori_loop(drained, items, drain, 0)
    for n in range(width // tile):
        out_copy(n).wait()


def body(sizes, tokens, in_gain, w_input, w_gate, conv_taps, w_rate, w_inlet, decay_param,
         decay_bias, out_gain, w_out):
    n_grp, n_sp, n_tp = sizes
    rows, width = tokens.shape
    channels = w_input.shape[1]
    heads, head = w_rate.shape[0], w_rate.shape[1]
    parts = head // LANES
    steps = heads * (rows // CHUNK)
    out_rows = rows // n_tp
    out_width = w_out.shape[1]
    shard = w_out.shape[0]
    quarter = shard // (2 * n_grp)
    pieces = quarter // max(16, quarter // 4)
    all_channels = channels * n_tp
    tile = 512 if out_width % 512 == 0 else 256
    hbm = pl.BlockSpec(memory_space=pl.ANY)
    dma = pltpu.SemaphoreType.DMA
    return pl.pallas_call(
        functools.partial(kernel, sizes),
        out_shape=jax.ShapeDtypeStruct((out_rows, out_width), BF16),
        in_specs=[hbm] * 11,
        out_specs=hbm,
        scratch_shapes=[
            pltpu.VMEM((1, width), F32),
            pltpu.VMEM(conv_taps.shape, F32),
            pltpu.VMEM((1, channels), F32),
            pltpu.VMEM((heads, rows), F32),
            pltpu.VMEM((1, channels), F32),
            pltpu.VMEM((16, width), BF16),
            pltpu.VMEM((rows, width), BF16),
            pltpu.VMEM((heads, width, 2 * head), BF16),
            pltpu.VMEM((all_channels, out_width), BF16),
            pltpu.VMEM((heads, head, 2 * head), BF16),
            pltpu.VMEM((rows, LANES), F32),
            pltpu.VMEM((parts, 8 * STRIDE, LANES), F32),
            pltpu.VMEM((parts, 8 * STRIDE, LANES), F32),
            pltpu.VMEM((CHUNK, head), BF16),
            pltpu.VMEM((CHUNK, 2 * head), F32),
            pltpu.VMEM((8 * STRIDE, LANES), F32),
            pltpu.VMEM((1, channels), F32),
            pltpu.VMEM((heads, parts, 8, LANES), F32),
            pltpu.VMEM((steps, parts, CHUNK, LANES), F32),
            pltpu.VMEM((steps, parts, CHUNK, LANES), F32),
            pltpu.VMEM((steps, parts, CHUNK, LANES), F32),
            pltpu.VMEM((steps, parts, 8, LANES), F32),
            pltpu.VMEM((steps, parts, 8, LANES), F32),
            pltpu.VMEM((parts, 8 * STRIDE, LANES), F32),
            pltpu.VMEM((heads, rows, head), BF16),
            pltpu.VMEM((n_tp * heads, out_rows, head), BF16),
            pltpu.VMEM((out_rows, out_width), F32),
            pltpu.VMEM((out_rows, out_width), BF16),
            pltpu.VMEM((16, width), BF16),
            pltpu.VMEM((heads * n_tp, 8, out_rows), F32),
            pltpu.VMEM((n_tp * heads, 8, out_rows), F32),
            pltpu.VMEM((heads, parts, 16, LANES), F32),
            pltpu.VMEM((heads * n_sp, parts, 16, LANES), F32),
            dma((rows // CHUNK,)),
            dma((2 * heads,)),
            dma,
            dma,
            dma,
            dma((2 * n_sp * pieces,)),
            dma((n_sp * pieces,)),
            dma((n_sp * pieces,)),
            dma((n_sp * pieces,)),
            dma((2 * n_sp * pieces,)),
            dma((2 * n_sp * pieces,)),
            dma((heads * n_sp,)),
            dma((heads * n_sp,)),
            dma((heads * n_tp,)),
            dma((heads * n_tp,)),
            dma((heads * n_tp,)),
            dma((heads * n_tp,)),
            dma((2 * heads,)),
            dma((out_width // tile,)),
            dma((7,)),
            dma,
        ],
        compiler_params=pltpu.CompilerParams(
            collective_id=0, has_side_effects=True, vmem_limit_bytes=62 * 1024 * 1024
        ),
    )(
        tokens, in_gain.reshape(1, width), w_input, w_gate, conv_taps, w_rate, w_inlet,
        decay_param.reshape(1, channels), decay_bias, out_gain.reshape(1, channels), w_out,
    )


def solution(mesh):
    sizes = (mesh.shape["grp"], mesh.shape["sp"], mesh.shape["tp"])
    return jax.shard_map(
        functools.partial(body, sizes),
        mesh=mesh,
        in_specs=(
            P(("grp", "sp"), None),
            P(),
            P(None, "tp"),
            P(None, "tp"),
            P(None, "tp"),
            P("tp", None, None),
            P("tp", None, None),
            P("tp"),
            P("tp", ("grp", "sp")),
            P("tp"),
            P("sp", None),
        ),
        out_specs=P(("grp", "sp", "tp"), None),
        check_vma=False,
    )
```

```python
import functools
import math
import jax
import jax.numpy as jnp
from jax import lax
from jax.experimental import pallas as pl
from jax.experimental.pallas import tpu as pltpu
from jax.sharding import PartitionSpec as P

MESH = pl.DeviceIdType.MESH
F32 = jnp.float32
BF16 = jnp.bfloat16
CHUNK = 256
SEG = CHUNK // 8
STRIDE = SEG + 8
LANES = 128
LAG = 6
FIRST = 1
EVERY = 3
BEHIND = 3
AHEAD = 7
EARLY = 3
BETWEEN = 1
REST = 4
LN2 = math.log(2.0)
GELU_A = math.sqrt(2.0 / math.pi)
GELU_B = GELU_A * 0.044715


def gelu_half(value):
    inner = value * (GELU_A + GELU_B * (value * value))
    return (0.25 * value) * (1.0 + jnp.tanh(inner))


def softplus_of_minus(value):
    small = jnp.exp(-jnp.abs(value))
    z = small / (2.0 + small)
    zz = z * z
    series = 1.0 / 15.0
    for n in (13, 11, 9, 7, 5, 3, 1):
        series = series * zz + 1.0 / n
    return jnp.maximum(-value, 0.0) + 2.0 * z * series


def spread(row):
    return jnp.broadcast_to(row, (8, row.shape[1]))


def columns_of(row):
    return jnp.broadcast_to(row, (LANES, row.shape[1])).T


def kernel(
    sizes,
    tokens, in_gain_h, w_input, w_gate, taps_h, w_rate, w_inlet, decay_h, bias_h, out_gain_h, w_out,
    out,
    in_gain, taps, decay_param, bias, out_gain, tail,
    x, w_in, w_all, gates_w, inv, proj, graw, conv, raw, bias_p, scale_row, before,
    state, prod, gate, pre_s, pre_p, natural, gated, arrived, total, halo,
    squares, squares_in, ends, ends_in,
    x_sem, w_sem, out_load_sem, halo_send, halo_recv, z_send, z_recv, y_send, y_recv,
    m_send, m_recv, end_send, end_recv, a_send, a_recv, q_send, q_recv, own_sem,
    small_sem, tail_sem,
):
    n_grp, n_sp, n_tp = sizes
    grp, sp, tp = lax.axis_index("grp"), lax.axis_index("sp"), lax.axis_index("tp")
    rows, width = tokens.shape
    heads, head = w_rate.shape[0], w_rate.shape[1]
    parts = head // LANES
    channels = heads * head
    reach = taps.shape[0] - 1
    chunks = rows // CHUNK
    steps = heads * chunks
    out_rows = rows // n_tp
    per_owner = out_rows // CHUNK
    shard = w_out.shape[0]
    quarter = shard // (2 * n_grp)
    piece = max(16, quarter // 4)
    pieces = quarter // piece
    items = (n_sp - 1) * pieces
    core = lax.rem(tp, 2)
    mate = tp + 1 - 2 * core
    across = 1 - grp

    def x_copy(i):
        at = pl.ds(pl.multiple_of(i * CHUNK, CHUNK), CHUNK)
        return pltpu.make_async_copy(tokens.at[at], x.at[at], x_sem.at[i])

    def w_copies(h):
        lanes = pl.ds(h * head, head)
        return (
            pltpu.make_async_copy(w_input.at[:, lanes], w_in.at[h, :, 0:head], w_sem.at[2 * h]),
            pltpu.make_async_copy(
                w_gate.at[:, lanes], w_in.at[h, :, head : 2 * head], w_sem.at[2 * h + 1]
            ),
        )

    out_load = pltpu.make_async_copy(
        w_out, w_all.at[pl.ds(pl.multiple_of(sp * shard, shard), shard)], out_load_sem
    )

    smalls = [
        pltpu.make_async_copy(source, target, small_sem.at[n])
        for n, (source, target) in enumerate((
            (in_gain_h, in_gain), (w_rate, gates_w.at[:, :, 0:head]),
            (w_inlet, gates_w.at[:, :, head : 2 * head]), (decay_h, decay_param),
            (bias_h, bias), (taps_h, taps), (out_gain_h, out_gain),
        ))
    ]
    ends_in[...] = jnp.zeros_like(ends_in)
    barrier = pltpu.get_barrier_semaphore()
    for d in range(1, n_sp):
        pl.semaphore_signal(
            barrier, inc=1, device_id={"sp": lax.rem(sp + d, n_sp)}, device_id_type=MESH
        )
    for k in range(1, n_tp):
        pl.semaphore_signal(
            barrier, inc=1, device_id={"tp": lax.rem(tp + k, n_tp)}, device_id_type=MESH
        )
    pl.semaphore_signal(barrier, inc=1, device_id={"grp": across}, device_id_type=MESH)

    smalls[0].start()
    for copy in w_copies(0):
        copy.start()
    halo_rows = halo.shape[0]
    tail_copy = pltpu.make_async_copy(
        tokens.at[pl.ds(rows - halo_rows, halo_rows)], tail, tail_sem
    )
    tail_copy.start()
    x_copy(0).start()
    for copy in smalls[1:]:
        copy.start()

    def remote(src, dst, send, recv, where):
        return pltpu.make_async_remote_copy(
            src_ref=src, dst_ref=dst, send_sem=send, recv_sem=recv,
            device_id=where, device_id_type=MESH,
        )

    halo_copy = remote(
        tail, halo, halo_send, halo_recv,
        {"sp": jnp.minimum(sp + 1, n_sp - 1)},
    )

    def w_rows(source, which, p):
        first = source * shard + which * quarter + p * piece
        return w_all.at[pl.ds(pl.multiple_of(first, piece), piece)]

    def which_of(other, owner):
        return (across if other else grp) * 2 + owner

    def own_copy(to_right, p):
        mine = which_of(False, core)
        first = pl.multiple_of(mine * quarter + p * piece, piece)
        return remote(
            w_out.at[pl.ds(first, piece)], w_rows(sp, mine, p),
            z_send.at[0 if to_right else 1], z_recv.at[sp * pieces + p],
            {"sp": jnp.minimum(sp + 1, n_sp - 1) if to_right else jnp.maximum(sp - 1, 0)},
        )

    def z_copy(source, p, to_right):
        at = w_rows(source, which_of(False, core), p)
        return remote(
            at, at, z_send.at[0 if to_right else 1], z_recv.at[source * pieces + p],
            {"sp": jnp.minimum(sp + 1, n_sp - 1) if to_right else jnp.maximum(sp - 1, 0)},
        )

    def y_copy(source, p, incoming=False):
        at = w_rows(source, which_of(incoming, core), p)
        slot = source * pieces + p
        return remote(at, at, y_send, y_recv.at[slot], {"grp": across})

    def m_copy(source, p, second, incoming=False):
        at = w_rows(source, which_of(second, 1 - core if incoming else core), p)
        slot = ((1 if second else 0) * n_sp + source) * pieces + p
        return remote(at, at, m_send, m_recv.at[slot], {"tp": mate})

    inner = jnp.minimum(sp, n_sp - 1 - sp)
    leftward = sp > n_sp - 1 - sp

    def source_of(b):
        d = jnp.where(b <= 2 * inner, (b + 1) // 2, b - inner)
        from_left = jnp.where(b <= 2 * inner, b % 2 == 1, leftward)
        return jnp.where(from_left, sp - d, sp + d)

    held = (1, 2) if heads > 1 else ()

    def each_source(n, action):
        d, p = 1 + n // pieces, n % pieces

        @pl.when(sp >= d)
        def _():
            action(sp - d, p, True)

        @pl.when(sp + d < n_sp)
        def _():
            action(sp + d, p, False)

    def onward(source, p, from_left, act):
        if from_left:
            pl.when(sp < n_sp - 1)(lambda: act(z_copy(source, p, True)))
        else:
            pl.when(sp > 0)(lambda: act(z_copy(source, p, False)))

    def take_z(source, p, from_left):
        z_copy(source, p, from_left).wait_recv()
        y_copy(source, p).start()
        m_copy(source, p, False).start()

    def take_y(source, p, from_left):
        y_copy(source, p, True).wait_recv()
        m_copy(source, p, True).start()

    def send_on(up, source, p, from_left):
        if up == from_left:
            onward(source, p, from_left, lambda copy: copy.start())

    def pump(n):
        @pl.when(n < items)
        def _():
            each_source(n, take_z)
            each_source(n, functools.partial(send_on, False))

        @pl.when(((n < min(held, default=0)) | (n > max(held, default=-1))) & (n < items))
        def _():
            each_source(n, functools.partial(send_on, True))

        @pl.when(n >= LAG)
        def _():
            each_source(n - LAG, take_y)

    def fold(h):
        def block(j, _):
            at = pl.ds(pl.multiple_of(j * CHUNK, CHUNK), CHUNK)
            gain = columns_of(in_gain[0:1, at])
            for c in range(2 * parts):
                lanes = slice(c * LANES, (c + 1) * LANES)
                w_in[h, at, lanes] = (w_in[h, at, lanes].astype(F32) * gain).astype(BF16)
            return 0

        lax.fori_loop(0, width // CHUNK, block, 0)

    def norm_of(chunk):
        as_float = chunk.astype(F32)
        return lax.rsqrt(jnp.mean(as_float * as_float, axis=1, keepdims=True) + 1e-06)

    def lanes_of(h, c):
        return pl.ds(pl.multiple_of(h * head + c * LANES, LANES), LANES)

    def project(s, sums):
        h, i = s // chunks, s % chunks
        at = pl.ds(pl.multiple_of(i * CHUNK, CHUNK), CHUNK)
        acc = jnp.dot(x[at, :], w_in[h], preferred_element_type=F32)
        if sums:
            scale = jnp.broadcast_to(norm_of(x[at, :]), (CHUNK, LANES))
            inv[at, :] = scale
        else:
            scale = inv[at, :]
        return acc, scale

    def keep(s, acc, scale):
        h, i = s // chunks, s % chunks
        for c in range(parts):
            last = proj[c, 7 * STRIDE + SEG : 8 * STRIDE, :]
            proj[c, 0:8, :] = jnp.where(i == 0, before[h, c], last)
            for g in range(8):
                at = slice(g * SEG, (g + 1) * SEG)
                block = acc[at, c * LANES : (c + 1) * LANES] * scale[at]
                proj[c, g * STRIDE + 8 : (g + 1) * STRIDE, :] = block
                if g < 7:
                    proj[c, (g + 1) * STRIDE : (g + 1) * STRIDE + 8, :] = block[SEG - 8 :]
                other = acc[at, head + c * LANES : head + (c + 1) * LANES] * scale[at]
                graw[c, g * STRIDE : g * STRIDE + SEG, :] = other

    def convolve(s):
        h, i = s // chunks, s % chunks
        for c in range(parts):
            lanes = lanes_of(h, c)
            tap = [spread(taps[k : k + 1, lanes]) for k in range(reach + 1)]
            window = [
                proj[c, pl.ds(8 - reach + j, 8, stride=STRIDE), :] for j in range(SEG + reach)
            ]
            done = []
            for k in range(SEG):
                summed = window[k] * tap[0]
                for j in range(1, reach + 1):
                    summed = summed + window[k + j] * tap[j]
                done.append(summed)
            for k in range(SEG):
                value = graw[c, pl.ds(k, 8, stride=STRIDE), :]
                gate[s, c, k * 8 : k * 8 + 8, :] = gelu_half(value)
            for k in range(0, SEG, 2):
                pair = jnp.concatenate(done[k : k + 2], axis=0).astype(BF16)
                conv[k * 8 : k * 8 + 16, c * LANES : (c + 1) * LANES] = pair
        row = bias[pl.ds(h, 1), pl.ds(pl.multiple_of(i * CHUNK, CHUNK), CHUNK)] * (1.0 / LN2)
        cols = columns_of(row)
        for g in range(8):
            bias_p[g * STRIDE : g * STRIDE + SEG, :] = cols[g * SEG : (g + 1) * SEG]
        raw[...] = jnp.dot(conv[...], gates_w[h], preferred_element_type=F32)

    sublane = lax.broadcasted_iota(jnp.int32, (8, LANES), 0)

    def elementwise(s, carry):
        h, i = s // chunks, s % chunks
        after = []
        for c in range(parts):
            scale = spread(scale_row[0:1, lanes_of(h, c)])
            lanes = slice(c * LANES, (c + 1) * LANES)
            st, pt = jnp.zeros((8, LANES), F32), jnp.ones((8, LANES), F32)
            for k in range(SEG):
                at = slice(k * 8, k * 8 + 8)
                if k % 2 == 0:
                    pair = conv[k * 8 : k * 8 + 16, lanes].astype(F32)
                value = pair[(k % 2) * 8 : (k % 2) * 8 + 8]
                shift = bias_p[pl.ds(k, 8, stride=STRIDE), :] + scale
                log2_decay = jnp.tanh(raw[at, lanes]) * scale + shift
                decay = jnp.exp2(log2_decay)
                left = jnp.tanh(log2_decay * -LN2) * (1.0 + decay * decay)
                inlet = raw[at, head + c * LANES : head + (c + 1) * LANES]
                drive = (
                    left * lax.rsqrt(jnp.maximum(left, 1e-37)) * ((1.0 + jnp.tanh(inlet)) * value)
                )
                st = decay * st + drive
                pt = decay * pt
                state[s, c, at, :] = st
                prod[s, c, at, :] = pt
            for d in (1, 2, 4):
                inside = sublane >= d
                st = st + pt * jnp.where(inside, pltpu.roll(st, d, 0), 0.0)
                pt = pt * jnp.where(inside, pltpu.roll(pt, d, 0), 1.0)
            s_in = jnp.where(i == 0, 0.0, carry[2 * c])
            p_in = jnp.where(i == 0, 1.0, carry[2 * c + 1])
            inside = sublane >= 1
            s_ex = jnp.where(inside, pltpu.roll(st, 1, 0), 0.0)
            p_ex = jnp.where(inside, pltpu.roll(pt, 1, 0), 1.0)
            pre_s[s, c] = s_ex + p_ex * s_in
            pre_p[s, c] = p_ex * p_in
            p_last = spread(pt[7:8])
            after += [spread(st[7:8]) + p_last * s_in, p_last * p_in]
        return tuple(after)

    def start_carry():
        zero, one = jnp.zeros((8, LANES), F32), jnp.ones((8, LANES), F32)
        return (zero, one) * parts

    def end_copy(h, d):
        k = h * n_sp + d
        return remote(
            ends.at[h], ends_in.at[k], end_send.at[k], end_recv.at[k],
            {"sp": jnp.minimum(sp + d, n_sp - 1)},
        )

    def send_ends(h, carry):
        for c in range(parts):
            ends[h, c, 0:8, :] = carry[2 * c]
            ends[h, c, 8:16, :] = carry[2 * c + 1]
        for d in range(1, n_sp):
            pl.when(sp + d < n_sp)(end_copy(h, d).start)

    def take_ends(h):
        carry = [jnp.zeros((8, LANES), F32)] * parts
        for d in range(n_sp - 1, 0, -1):
            pl.when(sp >= d)(end_copy(h, d).wait_recv)
            k = h * n_sp + d
            for c in range(parts):
                new = ends_in[k, c, 0:8, :] + ends_in[k, c, 8:16, :] * carry[c]
                carry[c] = jnp.where(d <= sp, new, carry[c])
        return carry

    def a_copy(h, k):
        to = lax.rem(tp + k, n_tp)
        at = pl.ds(pl.multiple_of(to * out_rows, out_rows), out_rows)
        slot = h * n_tp + k
        return remote(
            gated.at[h, at], arrived.at[tp * heads + h], a_send.at[slot], a_recv.at[slot],
            {"tp": to},
        )

    def q_copy(h, k):
        to = lax.rem(tp + k, n_tp)
        slot = h * n_tp + k
        return remote(
            squares.at[h * n_tp + to], squares_in.at[tp * heads + h],
            q_send.at[slot], q_recv.at[slot], {"tp": to},
        )

    def own_copies(h):
        at = pl.ds(pl.multiple_of(tp * out_rows, out_rows), out_rows)
        return (
            pltpu.make_async_copy(gated.at[h, at], arrived.at[tp * heads + h], own_sem.at[2 * h]),
            pltpu.make_async_copy(
                squares.at[h * n_tp + tp], squares_in.at[tp * heads + h], own_sem.at[2 * h + 1]
            ),
        )

    order = list(range(2, n_tp)) + [1, 0]

    def phase_b(h, carry):
        gains = [spread(out_gain[0:1, lanes_of(h, c)]) for c in range(parts)]

        def block(to, j):
            s = h * chunks + to * per_owner + j
            for c in range(parts):
                start = pre_s[s, c] + pre_p[s, c] * carry[c]
                for k in range(SEG):
                    at = slice(k * 8, k * 8 + 8)
                    full = state[s, c, at, :] + prod[s, c, at, :] * start
                    natural[c, pl.ds(k, 8, stride=STRIDE), :] = full * gate[s, c, at, :]
            first = pl.multiple_of(to * out_rows + j * CHUNK, CHUNK)
            sums = []
            for g in range(8):
                part = None
                for c in range(parts):
                    value = natural[c, g * STRIDE : g * STRIDE + SEG, :]
                    gain = jnp.concatenate([gains[c]] * (SEG // 8), axis=0)
                    into = pl.ds(pl.multiple_of(first + g * SEG, SEG), SEG)
                    gated[h, into, c * LANES : (c + 1) * LANES] = (value * gain).astype(BF16)
                    part = value * value if part is None else part + value * value
                sums.append(part)
            row = jnp.sum(jnp.concatenate(sums, axis=0).T, axis=0, keepdims=True)
            at = pl.ds(pl.multiple_of(j * CHUNK, CHUNK), CHUNK)
            squares[h * n_tp + to, :, at] = spread(row)

        def owner(n, _):
            k = lax.rem(n + 2, n_tp)
            k = jnp.where(n == n_tp - 2, 1, jnp.where(n == n_tp - 1, 0, k))
            to = lax.rem(tp + k, n_tp)

            def one(j, _):
                block(to, j)
                return 0

            lax.fori_loop(0, per_owner, one, 0)

            @pl.when(k == 0)
            def _():
                for copy in own_copies(h):
                    copy.start()

            @pl.when(k > 0)
            def _():
                a_copy(h, k).start()
                q_copy(h, k).start()

            return 0

        lax.fori_loop(0, n_tp, owner, 0)

    h_all = range(heads)
    smalls[0].wait()
    for copy in w_copies(0):
        copy.wait()
    for h in range(1, heads):
        for copy in w_copies(h):
            copy.start()
    x_copy(1).start()
    fold(0)
    tail_copy.wait()
    pl.semaphore_wait(barrier, n_sp - 1 + n_tp - 1 + 1)
    pl.when(sp < n_sp - 1)(halo_copy.start)
    for p in range(pieces):
        pl.when(sp < n_sp - 1)(own_copy(True, p).start)
        pl.when(sp > 0)(own_copy(False, p).start)
    x_copy(0).wait()
    acc, scale = project(0, True)
    for c in range(parts):
        proj[c, 7 * STRIDE + SEG : 8 * STRIDE, :] = jnp.zeros((8, LANES), F32)
    for copy in smalls[1:]:
        copy.wait()
    for h in h_all:
        gates_w[h] = gates_w[h] * 0.5
    scale_row[...] = softplus_of_minus(decay_param[...]) * (-4.0 / LN2)
    for h in range(1, heads):
        for copy in w_copies(h):
            copy.wait()
        fold(h)
    for i in range(2, chunks):
        x_copy(i).start()
    out_load.start()

    @pl.when(sp == 0)
    def _():
        before[...] = jnp.zeros_like(before)

    @pl.when(sp > 0)
    def _():
        halo_copy.wait_recv()
        halo_inv = norm_of(halo[...])
        for h in h_all:
            rows_before = jnp.dot(halo[...], w_in[h, :, 0:head], preferred_element_type=F32)
            rows_before = rows_before * halo_inv
            for c in range(parts):
                before[h, c] = rows_before[halo_rows - 8 :, c * LANES : (c + 1) * LANES]

    keep(0, acc, scale)
    x_copy(1).wait()
    acc, scale = project(1, True)
    convolve(0)
    keep(1, acc, scale)

    def finish_step(s, carry):
        @pl.when(s % chunks == chunks - 1)
        def _():
            send_ends(s // chunks, carry)

    def step(sums, s, carry):
        if sums:
            x_copy(s + 2).wait()

        if not sums and heads > 1:

            @pl.when(s == chunks)
            def _():
                for k in held:
                    each_source(k, functools.partial(send_on, True))

        @pl.when((s >= FIRST) & ((s - FIRST) % EVERY == 0))
        def _():
            pump((s - FIRST) // EVERY)

        if not sums and heads > 1:

            @pl.when((s >= chunks) & (s % chunks == BEHIND))
            def _():
                phase_b(s // chunks - 1, take_ends(s // chunks - 1))

        acc, scale = project(s + 2, sums)
        carry = elementwise(s, carry)
        convolve(s + 1)
        keep(s + 2, acc, scale)
        finish_step(s, carry)
        return carry

    carry = start_carry()
    carry = lax.fori_loop(0, chunks - 2, functools.partial(step, True), carry)
    carry = lax.fori_loop(chunks - 2, steps - 2, functools.partial(step, False), carry)
    done = -((FIRST - steps + 2) // EVERY)
    carry = elementwise(steps - 2, carry)
    convolve(steps - 1)
    carry = elementwise(steps - 1, carry)
    last = heads - 1
    send_ends(last, carry)
    before_last = min(done + EARLY, items + LAG)

    def pump_some(first, end):
        def one(n, _):
            pump(n)
            return 0

        lax.fori_loop(first, end, one, 0)

    pump_some(done, before_last)
    done = before_last
    phase_b(last, take_ends(last))
    out_load.wait()

    progressive = shard == channels
    tile = 512 if width % 512 == 0 else 256
    deep = min(shard, head)

    def wait_from(k, h):
        @pl.when(k == 0)
        def _():
            for copy in own_copies(h):
                copy.wait()

        @pl.when(k > 0)
        def _():
            a_copy(h, k).wait_recv()
            q_copy(h, k).wait_recv()

    def wait_mate(b):
        source = source_of(b)

        def one(p, _):
            m_copy(source, p, False, True).wait_recv()
            m_copy(source, p, True, True).wait_recv()
            return 0

        lax.fori_loop(0, pieces, one, 0)

    def prepare(b, h):
        source = source_of(b)
        if progressive:
            wait_from(lax.rem(tp - source + n_tp, n_tp), h)
        return source

    def multiply(source, columns, units):
        blocks = []
        for u in units:
            at = source * shard + u * deep
            from_col = pl.multiple_of(at % head, deep)
            blocks.append(arrived[at // head, :, pl.ds(from_col, deep)])
        left = jnp.concatenate(blocks, axis=1)
        first = pl.multiple_of(source * shard + units[0] * deep, deep)
        right = w_all[pl.ds(first, len(units) * deep), columns]
        return jnp.dot(left, right, preferred_element_type=F32)

    def columns_at(n):
        return pl.ds(pl.multiple_of(n * tile, tile), tile)

    if not progressive:
        for k in range(n_tp):
            for h in h_all:
                wait_from(k, h)
    units = shard // deep
    work = [(b, u) for u in range(units) for b in range(n_sp - 1)]
    ahead = max(done, AHEAD * items // 12)
    pump_some(done, ahead)
    cursor = ahead
    mates = {0}
    for index, (b, u) in enumerate(work):
        needed = b * pieces + LAG
        if index == n_sp - 1 and progressive:
            needed = max(needed, items + LAG - REST)
        if b > 0:
            pump_some(cursor, max(cursor, needed))
            cursor = max(cursor, needed)
        elif index > 0:
            pump_some(cursor, max(cursor, needed))
            cursor = max(cursor, needed)
        if b not in mates:
            wait_mate(b)
            mates.add(b)
        source = prepare(b, u)

        def partial_sum(n, _, source=source, index=index, u=u, cursor=cursor):
            columns = columns_at(n)
            value = multiply(source, columns, (u,))
            total[:, columns] = value if index == 0 else total[:, columns] + value

            @pl.when((n < BETWEEN) & (cursor + n < items + LAG))
            def _():
                pump(cursor + n)

            return 0

        lax.fori_loop(0, width // tile, partial_sum, 0)
        cursor = min(cursor + BETWEEN, items + LAG)
    def all_sent(semaphore, quarters):
        at = w_all.at[pl.ds(0, quarters * quarter)]
        remote(at, at, semaphore, semaphore, {"grp": across}).wait_send()

    pl.when(sp < n_sp - 1)(halo_copy.wait_send)
    for h in h_all:
        for d in range(1, n_sp):
            pl.when(sp + d < n_sp)(end_copy(h, d).wait_send)
        for k in range(1, n_tp):
            a_copy(h, k).wait_send()
            q_copy(h, k).wait_send()
    b = n_sp - 1
    if b > 0:
        pump_some(cursor, items + LAG)
        wait_mate(b)
    for u in range(units):
        source = prepare(b, u)
    row = squares_in[0]
    for k in range(1, n_tp * heads):
        row = row + squares_in[k]
    out_scale = lax.rsqrt(row[0:1] / (n_tp * heads * head) + 1e-06)
    scale_cols = jnp.broadcast_to(out_scale, (LANES, out_rows)).T

    def final(n, _):
        columns = columns_at(n)
        value = multiply(source, columns, tuple(range(units)))
        if n_sp > 1:
            value = value + total[:, columns]
        value = value * jnp.concatenate([scale_cols] * (tile // LANES), axis=1)
        out[:, columns] = value.astype(BF16)
        return 0

    lax.fori_loop(0, width // tile, final, 0)

    for k in range(n_sp - 1):
        pl.when(sp == k)(functools.partial(all_sent, z_send.at[0], k + 1))
        pl.when(sp == n_sp - 1 - k)(functools.partial(all_sent, z_send.at[1], k + 1))
    all_sent(y_send, n_sp - 1)
    all_sent(m_send, 2 * (n_sp - 1))


def body(sizes, tokens, in_gain, w_input, w_gate, conv_taps, w_rate, w_inlet, decay_param,
         decay_bias, out_gain, w_out):
    n_grp, n_sp, n_tp = sizes
    rows, width = tokens.shape
    channels = w_input.shape[1]
    heads, head = w_rate.shape[0], w_rate.shape[1]
    parts = head // LANES
    steps = heads * (rows // CHUNK)
    out_rows = rows // n_tp
    out_width = w_out.shape[1]
    shard = w_out.shape[0]
    quarter = shard // (2 * n_grp)
    pieces = quarter // max(16, quarter // 4)
    all_channels = channels * n_tp
    hbm = pl.BlockSpec(memory_space=pl.ANY)
    dma = pltpu.SemaphoreType.DMA
    return pl.pallas_call(
        functools.partial(kernel, sizes),
        out_shape=pltpu.VMEM((out_rows, out_width), BF16),
        in_specs=[hbm] * 11,
        out_specs=pl.BlockSpec(memory_space=pltpu.VMEM),
        scratch_shapes=[
            pltpu.VMEM((1, width), F32),
            pltpu.VMEM(conv_taps.shape, F32),
            pltpu.VMEM((1, channels), F32),
            pltpu.VMEM((heads, rows), F32),
            pltpu.VMEM((1, channels), F32),
            pltpu.VMEM((16, width), BF16),
            pltpu.VMEM((rows, width), BF16),
            pltpu.VMEM((heads, width, 2 * head), BF16),
            pltpu.VMEM((all_channels, out_width), BF16),
            pltpu.VMEM((heads, head, 2 * head), BF16),
            pltpu.VMEM((rows, LANES), F32),
            pltpu.VMEM((parts, 8 * STRIDE, LANES), F32),
            pltpu.VMEM((parts, 8 * STRIDE, LANES), F32),
            pltpu.VMEM((CHUNK, head), BF16),
            pltpu.VMEM((CHUNK, 2 * head), F32),
            pltpu.VMEM((8 * STRIDE, LANES), F32),
            pltpu.VMEM((1, channels), F32),
            pltpu.VMEM((heads, parts, 8, LANES), F32),
            pltpu.VMEM((steps, parts, CHUNK, LANES), F32),
            pltpu.VMEM((steps, parts, CHUNK, LANES), F32),
            pltpu.VMEM((steps, parts, CHUNK, LANES), F32),
            pltpu.VMEM((steps, parts, 8, LANES), F32),
            pltpu.VMEM((steps, parts, 8, LANES), F32),
            pltpu.VMEM((parts, 8 * STRIDE, LANES), F32),
            pltpu.VMEM((heads, rows, head), BF16),
            pltpu.VMEM((n_tp * heads, out_rows, head), BF16),
            pltpu.VMEM((out_rows, out_width), F32),
            pltpu.VMEM((16, width), BF16),
            pltpu.VMEM((heads * n_tp, 8, out_rows), F32),
            pltpu.VMEM((n_tp * heads, 8, out_rows), F32),
            pltpu.VMEM((heads, parts, 16, LANES), F32),
            pltpu.VMEM((heads * n_sp, parts, 16, LANES), F32),
            dma((rows // CHUNK,)),
            dma((2 * heads,)),
            dma,
            dma,
            dma,
            dma((2,)),
            dma((n_sp * pieces,)),
            dma,
            dma((n_sp * pieces,)),
            dma,
            dma((2 * n_sp * pieces,)),
            dma((heads * n_sp,)),
            dma((heads * n_sp,)),
            dma((heads * n_tp,)),
            dma((heads * n_tp,)),
            dma((heads * n_tp,)),
            dma((heads * n_tp,)),
            dma((2 * heads,)),
            dma((7,)),
            dma,
        ],
        compiler_params=pltpu.CompilerParams(
            collective_id=0, has_side_effects=True, vmem_limit_bytes=58 * 1024 * 1024
        ),
    )(*(
        pltpu.with_memory_space_constraint(array, pltpu.HBM)
        for array in (
            tokens, in_gain.reshape(1, width), w_input, w_gate, conv_taps, w_rate, w_inlet,
            decay_param.reshape(1, channels), decay_bias, out_gain.reshape(1, channels), w_out,
        )
    ))


def solution(mesh):
    sizes = (mesh.shape["grp"], mesh.shape["sp"], mesh.shape["tp"])
    return jax.shard_map(
        functools.partial(body, sizes),
        mesh=mesh,
        in_specs=(
            P(("grp", "sp"), None),
            P(),
            P(None, "tp"),
            P(None, "tp"),
            P(None, "tp"),
            P("tp", None, None),
            P("tp", None, None),
            P("tp"),
            P("tp", ("grp", "sp")),
            P("tp"),
            P("sp", None),
        ),
        out_specs=P(("grp", "sp", "tp"), None),
        check_vma=False,
    )
```

```python
import functools
import math
import jax
import jax.numpy as jnp
from jax import lax
from jax.experimental import pallas as pl
from jax.experimental.pallas import tpu as pltpu
from jax.sharding import PartitionSpec as P

MESH = pl.DeviceIdType.MESH
F32 = jnp.float32
BF16 = jnp.bfloat16
CHUNK = 256
SEG = CHUNK // 8
STRIDE = SEG + 8
LANES = 128
LAG = 6
FIRST = 1
EVERY = 3
BEHIND = 3
AHEAD = 8
EARLY = 3
BETWEEN = 1
REST = 4
LN2 = math.log(2.0)
GELU_A = math.sqrt(2.0 / math.pi)
GELU_B = GELU_A * 0.044715


def gelu_half(value):
    inner = value * (GELU_A + GELU_B * (value * value))
    return (0.25 * value) * (1.0 + jnp.tanh(inner))


def softplus_of_minus(value):
    small = jnp.exp(-jnp.abs(value))
    z = small / (2.0 + small)
    zz = z * z
    series = 1.0 / 15.0
    for n in (13, 11, 9, 7, 5, 3, 1):
        series = series * zz + 1.0 / n
    return jnp.maximum(-value, 0.0) + 2.0 * z * series


def spread(row):
    return jnp.broadcast_to(row, (8, row.shape[1]))


def columns_of(row):
    return jnp.broadcast_to(row, (LANES, row.shape[1])).T


def kernel(
    sizes,
    tokens, in_gain_h, w_input, w_gate, taps_h, w_rate, w_inlet, decay_h, bias_h, out_gain_h, w_out,
    out,
    in_gain, taps, decay_param, bias, out_gain, tail,
    x, w_in, w_all, gates_w, inv, proj, graw, conv, raw, bias_p, scale_row, before,
    state, prod, gate, pre_s, pre_p, natural, gated, arrived, total, halo,
    squares, squares_in, ends, ends_in,
    x_sem, w_sem, out_load_sem, halo_send, halo_recv, z_send, z_recv, y_send, y_recv,
    m_send, m_recv, end_send, end_recv, a_send, a_recv, q_send, q_recv, own_sem,
    small_sem, tail_sem,
):
    n_grp, n_sp, n_tp = sizes
    grp, sp, tp = lax.axis_index("grp"), lax.axis_index("sp"), lax.axis_index("tp")
    rows, width = tokens.shape
    heads, head = w_rate.shape[0], w_rate.shape[1]
    parts = head // LANES
    channels = heads * head
    reach = taps.shape[0] - 1
    chunks = rows // CHUNK
    steps = heads * chunks
    out_rows = rows // n_tp
    per_owner = out_rows // CHUNK
    shard = w_out.shape[0]
    quarter = shard // (2 * n_grp)
    piece = max(16, quarter // 4)
    pieces = quarter // piece
    items = (n_sp - 1) * pieces
    core = lax.rem(tp, 2)
    mate = tp + 1 - 2 * core
    across = 1 - grp
    side = lax.rem(tp // 2, 2)
    beside = tp + 2 - 4 * side
    over_tp = 0

    def x_copy(i):
        at = pl.ds(pl.multiple_of(i * CHUNK, CHUNK), CHUNK)
        return pltpu.make_async_copy(tokens.at[at], x.at[at], x_sem.at[i])

    def w_copies(h):
        lanes = pl.ds(h * head, head)
        return (
            pltpu.make_async_copy(w_input.at[:, lanes], w_in.at[h, :, 0:head], w_sem.at[2 * h]),
            pltpu.make_async_copy(
                w_gate.at[:, lanes], w_in.at[h, :, head : 2 * head], w_sem.at[2 * h + 1]
            ),
        )

    out_load = pltpu.make_async_copy(
        w_out, w_all.at[pl.ds(pl.multiple_of(sp * shard, shard), shard)], out_load_sem
    )

    smalls = [
        pltpu.make_async_copy(source, target, small_sem.at[n])
        for n, (source, target) in enumerate((
            (in_gain_h, in_gain), (w_rate, gates_w.at[:, :, 0:head]),
            (w_inlet, gates_w.at[:, :, head : 2 * head]), (decay_h, decay_param),
            (bias_h, bias), (taps_h, taps), (out_gain_h, out_gain),
        ))
    ]
    ends_in[...] = jnp.zeros_like(ends_in)
    barrier = pltpu.get_barrier_semaphore()
    for d in range(1, n_sp):
        pl.semaphore_signal(
            barrier, inc=1, device_id={"sp": lax.rem(sp + d, n_sp)}, device_id_type=MESH
        )
    for k in range(1, n_tp):
        pl.semaphore_signal(
            barrier, inc=1, device_id={"tp": lax.rem(tp + k, n_tp)}, device_id_type=MESH
        )
    pl.semaphore_signal(barrier, inc=1, device_id={"grp": across}, device_id_type=MESH)

    smalls[0].start()
    for copy in w_copies(0):
        copy.start()
    halo_rows = halo.shape[0]
    tail_copy = pltpu.make_async_copy(
        tokens.at[pl.ds(rows - halo_rows, halo_rows)], tail, tail_sem
    )
    tail_copy.start()
    x_copy(0).start()
    for copy in smalls[1:]:
        copy.start()

    def remote(src, dst, send, recv, where):
        return pltpu.make_async_remote_copy(
            src_ref=src, dst_ref=dst, send_sem=send, recv_sem=recv,
            device_id=where, device_id_type=MESH,
        )

    halo_copy = remote(
        tail, halo, halo_send, halo_recv,
        {"sp": jnp.minimum(sp + 1, n_sp - 1)},
    )

    def w_rows(source, which, p):
        first = source * shard + which * quarter + p * piece
        return w_all.at[pl.ds(pl.multiple_of(first, piece), piece)]

    def is_over_tp(source, p):
        return (p < over_tp) & (source > 0) & (source < n_sp - 1)

    def which_of(source, p, other, owner):
        near = jnp.where(is_over_tp(source, p), side, grp)
        return (1 - near if other else near) * 2 + owner

    def own_copy(to_right, p):
        mine = which_of(sp, p, False, core)
        first = pl.multiple_of(mine * quarter + p * piece, piece)
        return remote(
            w_out.at[pl.ds(first, piece)], w_rows(sp, mine, p),
            z_send.at[0 if to_right else 1], z_recv.at[sp * pieces + p],
            {"sp": jnp.minimum(sp + 1, n_sp - 1) if to_right else jnp.maximum(sp - 1, 0)},
        )

    def z_copy(source, p, to_right):
        at = w_rows(source, which_of(source, p, False, core), p)
        return remote(
            at, at, z_send.at[0 if to_right else 1], z_recv.at[source * pieces + p],
            {"sp": jnp.minimum(sp + 1, n_sp - 1) if to_right else jnp.maximum(sp - 1, 0)},
        )

    def y_copy(source, p, incoming=False):
        at = w_rows(source, which_of(source, p, incoming, core), p)
        slot = source * pieces + p
        turn = is_over_tp(source, p)
        to = {"grp": jnp.where(turn, grp, across), "tp": jnp.where(turn, beside, tp)}
        return remote(at, at, y_send, y_recv.at[slot], to)

    def m_copy(source, p, second, incoming=False):
        at = w_rows(source, which_of(source, p, second, 1 - core if incoming else core), p)
        slot = ((1 if second else 0) * n_sp + source) * pieces + p
        return remote(at, at, m_send, m_recv.at[slot], {"tp": mate})

    inner = jnp.minimum(sp, n_sp - 1 - sp)
    leftward = sp > n_sp - 1 - sp

    def source_of(b):
        d = jnp.where(b <= 2 * inner, (b + 1) // 2, b - inner)
        from_left = jnp.where(b <= 2 * inner, b % 2 == 1, leftward)
        return jnp.where(from_left, sp - d, sp + d)

    held = (1, 2) if heads > 1 else ()
    late = (4,) if heads > 1 else ()

    def each_source(n, action):
        d, p = 1 + n // pieces, n % pieces

        @pl.when(sp >= d)
        def _():
            action(sp - d, p, True)

        @pl.when(sp + d < n_sp)
        def _():
            action(sp + d, p, False)

    def onward(source, p, from_left, act):
        if from_left:
            pl.when(sp < n_sp - 1)(lambda: act(z_copy(source, p, True)))
        else:
            pl.when(sp > 0)(lambda: act(z_copy(source, p, False)))

    def take_z(source, p, from_left):
        z_copy(source, p, from_left).wait_recv()
        y_copy(source, p).start()
        m_copy(source, p, False).start()

    def take_y(source, p, from_left):
        y_copy(source, p, True).wait_recv()
        m_copy(source, p, True).start()

    def send_on(up, source, p, from_left):
        if up == from_left:
            onward(source, p, from_left, lambda copy: copy.start())

    def pump(n):
        @pl.when(n < items)
        def _():
            each_source(n, take_z)
            each_source(n, functools.partial(send_on, False))

        at_once = (n < min(held, default=0)) | (n > max(held, default=-1))
        at_once &= (n < min(late, default=0)) | (n > max(late, default=-1))

        @pl.when(at_once & (n < items))
        def _():
            each_source(n, functools.partial(send_on, True))

        @pl.when(n >= LAG)
        def _():
            each_source(n - LAG, take_y)

    def fold(h):
        together = 4 if width % (4 * CHUNK) == 0 else 1

        def block(j, _):
            for k in range(together):
                first = pl.multiple_of((j * together + k) * CHUNK, CHUNK)
                at = pl.ds(first, CHUNK)
                gain = columns_of(in_gain[0:1, at])
                for c in range(2 * parts):
                    lanes = slice(c * LANES, (c + 1) * LANES)
                    w_in[h, at, lanes] = (w_in[h, at, lanes].astype(F32) * gain).astype(BF16)
            return 0

        lax.fori_loop(0, width // (together * CHUNK), block, 0)

    def norm_of(chunk):
        as_float = chunk.astype(F32)
        return lax.rsqrt(jnp.mean(as_float * as_float, axis=1, keepdims=True) + 1e-06)

    def lanes_of(h, c):
        return pl.ds(pl.multiple_of(h * head + c * LANES, LANES), LANES)

    def project(s, sums):
        h, i = s // chunks, s % chunks
        at = pl.ds(pl.multiple_of(i * CHUNK, CHUNK), CHUNK)
        acc = jnp.dot(x[at, :], w_in[h], preferred_element_type=F32)
        if sums:
            scale = jnp.broadcast_to(norm_of(x[at, :]), (CHUNK, LANES))
            inv[at, :] = scale
        else:
            scale = inv[at, :]
        return acc, scale

    def keep(s, acc, scale):
        h, i = s // chunks, s % chunks
        for c in range(parts):
            last = proj[c, 7 * STRIDE + SEG : 8 * STRIDE, :]
            proj[c, 0:8, :] = jnp.where(i == 0, before[h, c], last)
            for g in range(8):
                at = slice(g * SEG, (g + 1) * SEG)
                block = acc[at, c * LANES : (c + 1) * LANES] * scale[at]
                proj[c, g * STRIDE + 8 : (g + 1) * STRIDE, :] = block
                if g < 7:
                    proj[c, (g + 1) * STRIDE : (g + 1) * STRIDE + 8, :] = block[SEG - 8 :]
                other = acc[at, head + c * LANES : head + (c + 1) * LANES] * scale[at]
                graw[c, g * STRIDE : g * STRIDE + SEG, :] = other

    def convolve(s):
        h, i = s // chunks, s % chunks
        for c in range(parts):
            lanes = lanes_of(h, c)
            tap = [spread(taps[k : k + 1, lanes]) for k in range(reach + 1)]
            window = [
                proj[c, pl.ds(8 - reach + j, 8, stride=STRIDE), :] for j in range(SEG + reach)
            ]
            done = []
            for k in range(SEG):
                summed = window[k] * tap[0]
                for j in range(1, reach + 1):
                    summed = summed + window[k + j] * tap[j]
                done.append(summed)
            for k in range(SEG):
                value = graw[c, pl.ds(k, 8, stride=STRIDE), :]
                gate[s, c, k * 8 : k * 8 + 8, :] = gelu_half(value)
            for k in range(0, SEG, 2):
                pair = jnp.concatenate(done[k : k + 2], axis=0).astype(BF16)
                conv[k * 8 : k * 8 + 16, c * LANES : (c + 1) * LANES] = pair
        row = bias[pl.ds(h, 1), pl.ds(pl.multiple_of(i * CHUNK, CHUNK), CHUNK)] * (1.0 / LN2)
        cols = columns_of(row)
        for g in range(8):
            bias_p[g * STRIDE : g * STRIDE + SEG, :] = cols[g * SEG : (g + 1) * SEG]
        raw[...] = jnp.dot(conv[...], gates_w[h], preferred_element_type=F32)

    sublane = lax.broadcasted_iota(jnp.int32, (8, LANES), 0)

    def elementwise(s, carry):
        h, i = s // chunks, s % chunks
        after = []
        for c in range(parts):
            scale = spread(scale_row[0:1, lanes_of(h, c)])
            lanes = slice(c * LANES, (c + 1) * LANES)
            st, pt = jnp.zeros((8, LANES), F32), jnp.ones((8, LANES), F32)
            for k in range(SEG):
                at = slice(k * 8, k * 8 + 8)
                if k % 2 == 0:
                    pair = conv[k * 8 : k * 8 + 16, lanes].astype(F32)
                value = pair[(k % 2) * 8 : (k % 2) * 8 + 8]
                shift = bias_p[pl.ds(k, 8, stride=STRIDE), :] + scale
                log2_decay = jnp.tanh(raw[at, lanes]) * scale + shift
                decay = jnp.exp2(log2_decay)
                left = jnp.tanh(log2_decay * -LN2) * (1.0 + decay * decay)
                inlet = raw[at, head + c * LANES : head + (c + 1) * LANES]
                drive = (
                    left * lax.rsqrt(jnp.maximum(left, 1e-37)) * ((1.0 + jnp.tanh(inlet)) * value)
                )
                st = decay * st + drive
                pt = decay * pt
                state[s, c, at, :] = st
                prod[s, c, at, :] = pt
            for d in (1, 2, 4):
                inside = sublane >= d
                st = st + pt * jnp.where(inside, pltpu.roll(st, d, 0), 0.0)
                pt = pt * jnp.where(inside, pltpu.roll(pt, d, 0), 1.0)
            s_in = jnp.where(i == 0, 0.0, carry[2 * c])
            p_in = jnp.where(i == 0, 1.0, carry[2 * c + 1])
            inside = sublane >= 1
            s_ex = jnp.where(inside, pltpu.roll(st, 1, 0), 0.0)
            p_ex = jnp.where(inside, pltpu.roll(pt, 1, 0), 1.0)
            pre_s[s, c] = s_ex + p_ex * s_in
            pre_p[s, c] = p_ex * p_in
            p_last = spread(pt[7:8])
            after += [spread(st[7:8]) + p_last * s_in, p_last * p_in]
        return tuple(after)

    def start_carry():
        zero, one = jnp.zeros((8, LANES), F32), jnp.ones((8, LANES), F32)
        return (zero, one) * parts

    def end_copy(h, d):
        k = h * n_sp + d
        return remote(
            ends.at[h], ends_in.at[k], end_send.at[k], end_recv.at[k],
            {"sp": jnp.minimum(sp + d, n_sp - 1)},
        )

    def send_ends(h, carry):
        for c in range(parts):
            ends[h, c, 0:8, :] = carry[2 * c]
            ends[h, c, 8:16, :] = carry[2 * c + 1]
        for d in range(1, n_sp):
            pl.when(sp + d < n_sp)(end_copy(h, d).start)

    def take_ends(h):
        carry = [jnp.zeros((8, LANES), F32)] * parts
        for d in range(n_sp - 1, 0, -1):
            pl.when(sp >= d)(end_copy(h, d).wait_recv)
            k = h * n_sp + d
            for c in range(parts):
                new = ends_in[k, c, 0:8, :] + ends_in[k, c, 8:16, :] * carry[c]
                carry[c] = jnp.where(d <= sp, new, carry[c])
        return carry

    def a_copy(h, k):
        to = lax.rem(tp + k, n_tp)
        at = pl.ds(pl.multiple_of(to * out_rows, out_rows), out_rows)
        slot = h * n_tp + k
        return remote(
            gated.at[h, at], arrived.at[tp * heads + h], a_send.at[slot], a_recv.at[slot],
            {"tp": to},
        )

    def q_copy(h, k):
        to = lax.rem(tp + k, n_tp)
        slot = h * n_tp + k
        return remote(
            squares.at[h * n_tp + to], squares_in.at[tp * heads + h],
            q_send.at[slot], q_recv.at[slot], {"tp": to},
        )

    def own_copies(h):
        at = pl.ds(pl.multiple_of(tp * out_rows, out_rows), out_rows)
        return (
            pltpu.make_async_copy(gated.at[h, at], arrived.at[tp * heads + h], own_sem.at[2 * h]),
            pltpu.make_async_copy(
                squares.at[h * n_tp + tp], squares_in.at[tp * heads + h], own_sem.at[2 * h + 1]
            ),
        )

    order = list(range(2, n_tp)) + [1, 0]

    def phase_b(h, carry):
        gains = [spread(out_gain[0:1, lanes_of(h, c)]) for c in range(parts)]

        def block(to, j):
            s = h * chunks + to * per_owner + j
            for c in range(parts):
                start = pre_s[s, c] + pre_p[s, c] * carry[c]
                for k in range(SEG):
                    at = slice(k * 8, k * 8 + 8)
                    full = state[s, c, at, :] + prod[s, c, at, :] * start
                    natural[c, pl.ds(k, 8, stride=STRIDE), :] = full * gate[s, c, at, :]
            first = pl.multiple_of(to * out_rows + j * CHUNK, CHUNK)
            sums = []
            for g in range(8):
                part = None
                for c in range(parts):
                    value = natural[c, g * STRIDE : g * STRIDE + SEG, :]
                    gain = jnp.concatenate([gains[c]] * (SEG // 8), axis=0)
                    into = pl.ds(pl.multiple_of(first + g * SEG, SEG), SEG)
                    gated[h, into, c * LANES : (c + 1) * LANES] = (value * gain).astype(BF16)
                    part = value * value if part is None else part + value * value
                sums.append(part)
            row = jnp.sum(jnp.concatenate(sums, axis=0).T, axis=0, keepdims=True)
            at = pl.ds(pl.multiple_of(j * CHUNK, CHUNK), CHUNK)
            squares[h * n_tp + to, :, at] = spread(row)

        def owner(n, _):
            k = lax.rem(n + 2, n_tp)
            k = jnp.where(n == n_tp - 2, 1, jnp.where(n == n_tp - 1, 0, k))
            to = lax.rem(tp + k, n_tp)

            def one(j, _):
                block(to, j)
                return 0

            lax.fori_loop(0, per_owner, one, 0)

            @pl.when(k == 0)
            def _():
                for copy in own_copies(h):
                    copy.start()

            @pl.when(k > 0)
            def _():
                a_copy(h, k).start()
                q_copy(h, k).start()

            return 0

        lax.fori_loop(0, n_tp, owner, 0)

    h_all = range(heads)
    smalls[0].wait()
    for copy in w_copies(0):
        copy.wait()
    for h in range(1, heads):
        for copy in w_copies(h):
            copy.start()
    x_copy(1).start()
    fold(0)
    tail_copy.wait()
    pl.semaphore_wait(barrier, n_sp - 1 + n_tp - 1 + 1)
    pl.when(sp < n_sp - 1)(halo_copy.start)
    for p in range(pieces):
        pl.when(sp < n_sp - 1)(own_copy(True, p).start)
        pl.when(sp > 0)(own_copy(False, p).start)
    x_copy(0).wait()
    acc, scale = project(0, True)
    for c in range(parts):
        proj[c, 7 * STRIDE + SEG : 8 * STRIDE, :] = jnp.zeros((8, LANES), F32)
    for copy in smalls[1:]:
        copy.wait()
    for h in h_all:
        gates_w[h] = gates_w[h] * 0.5
    scale_row[...] = softplus_of_minus(decay_param[...]) * (-4.0 / LN2)
    for h in range(1, heads):
        for copy in w_copies(h):
            copy.wait()
        fold(h)
    for i in range(2, chunks):
        x_copy(i).start()
    out_load.start()

    @pl.when(sp == 0)
    def _():
        before[...] = jnp.zeros_like(before)

    @pl.when(sp > 0)
    def _():
        halo_copy.wait_recv()
        halo_inv = norm_of(halo[...])
        for h in h_all:
            rows_before = jnp.dot(halo[...], w_in[h, :, 0:head], preferred_element_type=F32)
            rows_before = rows_before * halo_inv
            for c in range(parts):
                before[h, c] = rows_before[halo_rows - 8 :, c * LANES : (c + 1) * LANES]

    keep(0, acc, scale)
    x_copy(1).wait()
    acc, scale = project(1, True)
    convolve(0)
    keep(1, acc, scale)

    def finish_step(s, carry):
        @pl.when(s % chunks == chunks - 1)
        def _():
            send_ends(s // chunks, carry)

    def step(sums, s, carry):
        if sums:
            x_copy(s + 2).wait()

        if not sums and heads > 1:

            @pl.when((s >= chunks) & (s % chunks == BEHIND))
            def _():
                phase_b(s // chunks - 1, take_ends(s // chunks - 1))

        if not sums and heads > 1:

            @pl.when(s == chunks)
            def _():
                for k in held:
                    each_source(k, functools.partial(send_on, True))

        @pl.when((s >= FIRST) & ((s - FIRST) % EVERY == 0))
        def _():
            pump((s - FIRST) // EVERY)

        acc, scale = project(s + 2, sums)
        carry = elementwise(s, carry)
        convolve(s + 1)
        keep(s + 2, acc, scale)
        finish_step(s, carry)
        return carry

    carry = start_carry()
    carry = lax.fori_loop(0, chunks - 2, functools.partial(step, True), carry)
    carry = lax.fori_loop(chunks - 2, steps - 2, functools.partial(step, False), carry)
    done = -((FIRST - steps + 2) // EVERY)
    carry = elementwise(steps - 2, carry)
    convolve(steps - 1)
    carry = elementwise(steps - 1, carry)
    last = heads - 1
    send_ends(last, carry)
    before_last = min(done + EARLY, items + LAG)
    for k in late:
        each_source(k, functools.partial(send_on, True))

    def pump_some(first, end):
        def one(n, _):
            pump(n)
            return 0

        lax.fori_loop(first, end, one, 0)

    pump_some(done, before_last)
    done = before_last
    phase_b(last, take_ends(last))
    out_load.wait()

    progressive = shard == channels
    tile = 512 if width % 512 == 0 else 256
    deep = min(shard, head)

    def wait_from(k, h):
        @pl.when(k == 0)
        def _():
            for copy in own_copies(h):
                copy.wait()

        @pl.when(k > 0)
        def _():
            a_copy(h, k).wait_recv()
            q_copy(h, k).wait_recv()

    def wait_mate(b):
        source = source_of(b)

        def one(p, _):
            m_copy(source, p, False, True).wait_recv()
            m_copy(source, p, True, True).wait_recv()
            return 0

        lax.fori_loop(0, pieces, one, 0)

    def prepare(source, h):
        if progressive:
            wait_from(lax.rem(tp - source + n_tp, n_tp), h)
        return source

    def multiply(source, columns, units):
        blocks = []
        for u in units:
            at = source * shard + u * deep
            from_col = pl.multiple_of(at % head, deep)
            blocks.append(arrived[at // head, :, pl.ds(from_col, deep)])
        left = jnp.concatenate(blocks, axis=1)
        first = pl.multiple_of(source * shard + units[0] * deep, deep)
        right = w_all[pl.ds(first, len(units) * deep), columns]
        return jnp.dot(left, right, preferred_element_type=F32)

    def columns_at(n):
        return pl.ds(pl.multiple_of(n * tile, tile), tile)

    if not progressive:
        for k in range(n_tp):
            for h in h_all:
                wait_from(k, h)
    units = shard // deep
    end = source_of(n_sp - 1)
    base = 2 * (tp // 2)
    end_at = lax.rem(end - base + n_sp, n_sp) if progressive else 0

    def source_for(b, u):
        if u == 0 or not progressive:
            return source_of(b)
        return lax.rem(base + jnp.where(b < end_at, b, b + 1), n_sp)

    work = [(b, u) for u in range(units) for b in range(n_sp - 1)]
    ahead = max(done, AHEAD * items // 12)
    pump_some(done, ahead)
    cursor = ahead
    mates = {0}
    for index, (b, u) in enumerate(work):
        needed = b * pieces + LAG
        if index == n_sp - 1 and progressive:
            needed = max(needed, items + LAG - REST)
        if b > 0:
            pump_some(cursor, max(cursor, needed))
            cursor = max(cursor, needed)
        elif index > 0:
            pump_some(cursor, max(cursor, needed))
            cursor = max(cursor, needed)
        if b not in mates:
            wait_mate(b)
            mates.add(b)
        source = prepare(source_for(b, u), u)

        def partial_sum(n, _, source=source, index=index, u=u, cursor=cursor):
            columns = columns_at(n)
            value = multiply(source, columns, (u,))
            total[:, columns] = value if index == 0 else total[:, columns] + value

            @pl.when((n < BETWEEN) & (cursor + n < items + LAG))
            def _():
                pump(cursor + n)

            return 0

        lax.fori_loop(0, width // tile, partial_sum, 0)
        cursor = min(cursor + BETWEEN, items + LAG)
    def all_sent(semaphore, quarters):
        at = w_all.at[pl.ds(0, quarters * quarter)]
        remote(at, at, semaphore, semaphore, {"grp": across}).wait_send()

    pl.when(sp < n_sp - 1)(halo_copy.wait_send)
    for h in h_all:
        for d in range(1, n_sp):
            pl.when(sp + d < n_sp)(end_copy(h, d).wait_send)
        for k in range(1, n_tp):
            a_copy(h, k).wait_send()
            q_copy(h, k).wait_send()
    b = n_sp - 1
    if b > 0:
        pump_some(cursor, items + LAG)
        wait_mate(b)
    for u in range(units):
        source = prepare(source_of(b), u)
    row = squares_in[0]
    for k in range(1, n_tp * heads):
        row = row + squares_in[k]
    out_scale = lax.rsqrt(row[0:1] / (n_tp * heads * head) + 1e-06)
    scale_cols = jnp.broadcast_to(out_scale, (LANES, out_rows)).T

    def final(n, _):
        columns = columns_at(n)
        value = multiply(source, columns, tuple(range(units)))
        if n_sp > 1:
            value = value + total[:, columns]
        value = value * jnp.concatenate([scale_cols] * (tile // LANES), axis=1)
        out[:, columns] = value.astype(BF16)
        return 0

    lax.fori_loop(0, width // tile, final, 0)

    for k in range(n_sp - 1):
        pl.when(sp == k)(functools.partial(all_sent, z_send.at[0], k + 1))
        pl.when(sp == n_sp - 1 - k)(functools.partial(all_sent, z_send.at[1], k + 1))
    all_sent(y_send, n_sp - 1)
    all_sent(m_send, 2 * (n_sp - 1))


def body(sizes, tokens, in_gain, w_input, w_gate, conv_taps, w_rate, w_inlet, decay_param,
         decay_bias, out_gain, w_out):
    n_grp, n_sp, n_tp = sizes
    rows, width = tokens.shape
    channels = w_input.shape[1]
    heads, head = w_rate.shape[0], w_rate.shape[1]
    parts = head // LANES
    steps = heads * (rows // CHUNK)
    out_rows = rows // n_tp
    out_width = w_out.shape[1]
    shard = w_out.shape[0]
    quarter = shard // (2 * n_grp)
    pieces = quarter // max(16, quarter // 4)
    all_channels = channels * n_tp
    hbm = pl.BlockSpec(memory_space=pl.ANY)
    dma = pltpu.SemaphoreType.DMA
    return pl.pallas_call(
        functools.partial(kernel, sizes),
        out_shape=pltpu.VMEM((out_rows, out_width), BF16),
        in_specs=[hbm] * 11,
        out_specs=pl.BlockSpec(memory_space=pltpu.VMEM),
        scratch_shapes=[
            pltpu.VMEM((1, width), F32),
            pltpu.VMEM(conv_taps.shape, F32),
            pltpu.VMEM((1, channels), F32),
            pltpu.VMEM((heads, rows), F32),
            pltpu.VMEM((1, channels), F32),
            pltpu.VMEM((16, width), BF16),
            pltpu.VMEM((rows, width), BF16),
            pltpu.VMEM((heads, width, 2 * head), BF16),
            pltpu.VMEM((all_channels, out_width), BF16),
            pltpu.VMEM((heads, head, 2 * head), BF16),
            pltpu.VMEM((rows, LANES), F32),
            pltpu.VMEM((parts, 8 * STRIDE, LANES), F32),
            pltpu.VMEM((parts, 8 * STRIDE, LANES), F32),
            pltpu.VMEM((CHUNK, head), BF16),
            pltpu.VMEM((CHUNK, 2 * head), F32),
            pltpu.VMEM((8 * STRIDE, LANES), F32),
            pltpu.VMEM((1, channels), F32),
            pltpu.VMEM((heads, parts, 8, LANES), F32),
            pltpu.VMEM((steps, parts, CHUNK, LANES), F32),
            pltpu.VMEM((steps, parts, CHUNK, LANES), F32),
            pltpu.VMEM((steps, parts, CHUNK, LANES), F32),
            pltpu.VMEM((steps, parts, 8, LANES), F32),
            pltpu.VMEM((steps, parts, 8, LANES), F32),
            pltpu.VMEM((parts, 8 * STRIDE, LANES), F32),
            pltpu.VMEM((heads, rows, head), BF16),
            pltpu.VMEM((n_tp * heads, out_rows, head), BF16),
            pltpu.VMEM((out_rows, out_width), F32),
            pltpu.VMEM((16, width), BF16),
            pltpu.VMEM((heads * n_tp, 8, out_rows), F32),
            pltpu.VMEM((n_tp * heads, 8, out_rows), F32),
            pltpu.VMEM((heads, parts, 16, LANES), F32),
            pltpu.VMEM((heads * n_sp, parts, 16, LANES), F32),
            dma((rows // CHUNK,)),
            dma((2 * heads,)),
            dma,
            dma,
            dma,
            dma((2,)),
            dma((n_sp * pieces,)),
            dma,
            dma((n_sp * pieces,)),
            dma,
            dma((2 * n_sp * pieces,)),
            dma((heads * n_sp,)),
            dma((heads * n_sp,)),
            dma((heads * n_tp,)),
            dma((heads * n_tp,)),
            dma((heads * n_tp,)),
            dma((heads * n_tp,)),
            dma((2 * heads,)),
            dma((7,)),
            dma,
        ],
        compiler_params=pltpu.CompilerParams(
            collective_id=0, has_side_effects=True, vmem_limit_bytes=58 * 1024 * 1024
        ),
    )(*(
        pltpu.with_memory_space_constraint(array, pltpu.HBM)
        for array in (
            tokens, in_gain.reshape(1, width), w_input, w_gate, conv_taps, w_rate, w_inlet,
            decay_param.reshape(1, channels), decay_bias, out_gain.reshape(1, channels), w_out,
        )
    ))


def solution(mesh):
    sizes = (mesh.shape["grp"], mesh.shape["sp"], mesh.shape["tp"])
    return jax.shard_map(
        functools.partial(body, sizes),
        mesh=mesh,
        in_specs=(
            P(("grp", "sp"), None),
            P(),
            P(None, "tp"),
            P(None, "tp"),
            P(None, "tp"),
            P("tp", None, None),
            P("tp", None, None),
            P("tp"),
            P("tp", ("grp", "sp")),
            P("tp"),
            P("sp", None),
        ),
        out_specs=P(("grp", "sp", "tp"), None),
        check_vma=False,
    )
```
